256 devices in a mesh: rep: 2 (over z_hi), fs: 16 (over z_lo, y), tp: 8 (over x, core).
Axes of the slice: x: 4, y: 4, z: 8 (z_hi: 2, z_lo: 4; z = z_hi * 4 + z_lo), core: 2. Of those that a mesh axis runs over, the one named last changes fastest.
Arguments:
- block_input: bfloat16 [16384, 2048], P(('rep', 'fs', 'tp')), may hold values from -6 to 6
- pre_gain: float32 [2048], replicated, may hold values from 0.1 to 1.9
- post_gain: float32 [2048], replicated, may hold values from 0.1 to 1.9
- gate_saved: bfloat16 [16384, 5632], P(('rep', 'fs'), 'tp'), may hold values from -8 to 8
- up_saved: bfloat16 [16384, 5632], P(('rep', 'fs'), 'tp'), may hold values from -6 to 6
- branch_saved: bfloat16 [16384, 2048], P(('rep', 'fs', 'tp')), may hold values from -6 to 6
- out_cotangent: bfloat16 [16384, 2048], P(('rep', 'fs', 'tp')), may hold values from -24 to 24
- gate_weight: bfloat16 [2048, 5632], P('fs', 'tp'), may hold values from -0.125 to 0.125
- up_weight: bfloat16 [2048, 5632], P('fs', 'tp'), may hold values from -0.125 to 0.125
- down_weight: bfloat16 [2048, 5632], P('fs', 'tp'), may hold values from -0.078125 to 0.078125
Outputs:
- input_grad: bfloat16 [16384, 2048], P(('rep', 'fs', 'tp'))
- gate_grad: float32 [2048, 5632], P('fs', 'tp')
- up_grad: float32 [2048, 5632], P('fs', 'tp')
- down_grad: float32 [2048, 5632], P('fs', 'tp')
The draws below stay inside these ranges and needn't reach their ends.
All inputs are finite; a program needn't handle non-finite values.
Results may differ from the reference program's by a relative error of at most 0.018.
Values may be sent and summed in bfloat16 or wider, within the bound.
A program may use at most 128 MiB of HBM per device.

```python
import jax
import jax.numpy as jnp
from jax import lax

D = 2048
FF = 5632
TOKENS = 16384
N_TP = 8


def spiked(array, key, source, target, shards_of, factor):
    owner, partner = [(jnp.arange(array.shape[position]) // (array.shape[position] // shards_of)).reshape([-1 if axis == position else 1 for axis in range(array.ndim)]) for position in (source, target)]
    chosen = jax.random.permutation(key, shards_of)[partner]
    strong = (owner == chosen) | (owner == (partner + shards_of // 2) % shards_of)
    return jnp.where(strong, factor * array, array)


def shard_levels(key, dims, cuts, least, high):
    def one(position, parts):
        draws = jax.random.uniform(jax.random.fold_in(jax.random.fold_in(key, 6), position), (parts,), jnp.float32, least / len(cuts), high / len(cuts))
        return jnp.repeat(jnp.exp(draws), dims[position] // parts).reshape((-1,) + (1,) * (len(dims) - position - 1))

    factor_of = one(*cuts[0])
    for cut in cuts[1:]:
        factor_of = factor_of * one(*cut)
    return factor_of


def centred(key, shape, deviation, reach, pieces=(), dtype=jnp.bfloat16):
    factor_of = shard_levels(key, shape, pieces, -0.22, 0.18) if pieces else 1.0
    values = jax.random.normal(key, shape, jnp.float32) * deviation * factor_of
    return jnp.minimum(jnp.maximum(values, -reach), reach).astype(dtype)


def bell_draw_with(stream_key, dims, deviation, bound, pieces, heavy, dtype=jnp.bfloat16):
    drawn = deviation * jax.random.normal(stream_key, dims, jnp.float32)
    if pieces:
        drawn = drawn * shard_levels(stream_key, dims, pieces, -0.22, 0.18)
    return jnp.clip(spiked(drawn, jax.random.fold_in(stream_key, 3), *heavy), -bound, bound).astype(dtype)


def setup_inputs(seed: int = 0) -> dict:
    streams_of = jax.random.split(jax.random.key(seed), 11)
    return {
        "block_input": centred(streams_of[0], (TOKENS, D), 1.0, 6.0, ((0, 256),)),
        "pre_gain": jnp.clip(1.0 + 0.18 * jax.random.normal(streams_of[1], (D,), jnp.float32), 0.1, 1.9),
        "post_gain": jnp.clip(1.0 + 0.18 * jax.random.normal(streams_of[2], (D,), jnp.float32), 0.1, 1.9),
        "gate_saved": centred(streams_of[3], (TOKENS, FF), 1.5, 8.0, ((0, 32), (1, 8))),
        "up_saved": centred(streams_of[4], (TOKENS, FF), 1.0, 6.0, ((0, 32), (1, 8))),
        "branch_saved": centred(streams_of[5], (TOKENS, D), 1.0, 6.0, ((0, 256),)),
        "out_cotangent": bell_draw_with(streams_of[6], (TOKENS, D), 1.0, 24.0, ((0, 256),), (0, 1, 256, 6.0)),
        "gate_weight": centred(streams_of[7], (D, FF), D ** -0.5, 0.125, ((0, 16), (1, 8))),
        "up_weight": centred(streams_of[8], (D, FF), D ** -0.5, 0.125, ((0, 16), (1, 8))),
        "down_weight": centred(streams_of[9], (D, FF), FF ** -0.5, 0.078125, ((0, 16), (1, 8))),
    }


eps = 1e-06

def contract_rows(left, right):
    return lax.dot_general(left, right, (((0,), (0,)), ((), ())), preferred_element_type=jnp.float32)

def contract_cols(left, right):
    return lax.dot_general(left, right, (((1,), (1,)), ((), ())), preferred_element_type=jnp.float32)

def reference(block_input, pre_gain, post_gain, gate_saved, up_saved, branch_saved, out_cotangent, gate_weight, up_weight, down_weight):
    xfull = block_input.astype(jnp.float32)
    inv_x = lax.rsqrt(lax.optimization_barrier(jnp.mean(xfull * xfull, axis=-1, keepdims=True)) + eps)
    normed = (xfull * inv_x * pre_gain).astype(jnp.bfloat16)
    branch = branch_saved.astype(jnp.float32)
    inv_b = lax.rsqrt(lax.optimization_barrier(jnp.mean(branch * branch, axis=-1, keepdims=True)) + eps)
    upstream = 0.5 * out_cotangent.astype(jnp.float32) * post_gain
    branch_grad = (inv_b * upstream - branch * inv_b ** 3 * lax.optimization_barrier(jnp.mean(upstream * branch, axis=-1, keepdims=True))).astype(jnp.bfloat16)
    gate_f = gate_saved.astype(jnp.float32)
    up_f = up_saved.astype(jnp.float32)
    sigma = jax.nn.sigmoid(gate_f)
    silu_gate = gate_f * sigma
    hidden = (silu_gate * up_f).astype(jnp.bfloat16)
    hidden_grad = jnp.dot(branch_grad, down_weight, preferred_element_type=jnp.float32)
    gate_cot = (hidden_grad * up_f * sigma * (1.0 + gate_f * (1.0 - sigma))).astype(jnp.bfloat16)
    up_cot = (hidden_grad * silu_gate).astype(jnp.bfloat16)
    width = FF // N_TP
    normed_grad = jnp.zeros(xfull.shape, jnp.float32)
    for group in range(N_TP):
        lo = group * width
        partial_sum = contract_cols(gate_cot[:, lo:lo + width], gate_weight[:, lo:lo + width])
        partial_sum = partial_sum + contract_cols(up_cot[:, lo:lo + width], up_weight[:, lo:lo + width])
        normed_grad = normed_grad + lax.optimization_barrier(partial_sum.astype(jnp.bfloat16)).astype(jnp.float32)
    scaled = normed_grad * pre_gain
    input_grad = out_cotangent.astype(jnp.float32) + inv_x * scaled - xfull * inv_x ** 3 * lax.optimization_barrier(jnp.mean(scaled * xfull, axis=-1, keepdims=True))
    gate_grad = contract_rows(normed, gate_cot)
    up_grad = contract_rows(normed, up_cot)
    down_grad = contract_rows(branch_grad, hidden)
    return (input_grad.astype(jnp.bfloat16), gate_grad, up_grad, down_grad)
```

```python
import jax
import jax.numpy as jnp
from jax import lax
from jax.experimental import pallas as pl
from jax.experimental.pallas import tpu as pltpu
from jax.sharding import PartitionSpec as P

MESH = pl.DeviceIdType.MESH
bf16, f32 = jnp.bfloat16, jnp.float32
eps = 1e-06

H = 704
A, B = (0, 352), (352, 352)
QA, QB = ((0, 176), (176, 176)), ((352, 176), (528, 176))
P0, P1 = (0, 256), (256, 256)
Q0, Q1 = (0, 96), (96, 96)
QS = 512
N_SEM = 224


def ds(r):
    return pl.ds(r[0], r[1])


def mod(a, n):
    return lax.rem(a + n, n)


def kernel(
    x_ref, pre_ref, post_ref, gs_ref, us_ref, br_ref, oc_ref, gw_ref, uw_ref, dw_ref,
    ig_ref, gg_ref, ug_ref, dg_ref,
    W, R, G, RY1, RYa, RYb, RZ1, RZa, RZb, SY1, SYa, SYb, SZ1, SZa, SZb,
    T, XF, XR, silu, dgate, hid, cot, cotT, NG, NS, NX1, NXa, NXb, ssem, rsem,
):
    rep, fs, tp = lax.axis_index("rep"), lax.axis_index("fs"), lax.axis_index("tp")
    zl, y = fs // 4, fs % 4
    z = rep * 4 + zl
    x, core = tp // 2, tp % 2
    ym, yp, y2 = mod(y - 1, 4), mod(y + 1, 4), mod(y + 2, 4)
    zm, zp, z2 = mod(zl - 1, 4), mod(zl + 1, 4), mod(zl + 2, 4)
    xm, xp, x2 = mod(x - 1, 4), mod(x + 1, 4), mod(x + 2, 4)

    def zdev(d):
        zz = mod(z + d, 8)
        return {"rep": zz // 4, "fs": (zz % 4) * 4 + y}

    dev = {
        "y+": {"fs": zl * 4 + yp},
        "y-": {"fs": zl * 4 + ym},
        "z+": zdev(1),
        "z-": zdev(-1),
        "zz+": zdev(2),
        "zz-": zdev(-2),
        "x+": {"tp": xp * 2 + core},
        "x-": {"tp": xm * 2 + core},
        "s": {"tp": x * 2 + 1 - core},
    }

    barrier = pltpu.get_barrier_semaphore()
    for name in dev:
        pl.semaphore_signal(barrier, inc=1, device_id=dev[name], device_id_type=MESH)

    ids = {}
    sends = []

    def number(key):
        return ids.setdefault(key, len(ids))

    def send(key, src, dst, to):
        k = number(key)
        c = pltpu.make_async_remote_copy(
            src_ref=src, dst_ref=dst, send_sem=ssem.at[k], recv_sem=rsem.at[k],
            device_id=dev[to], device_id_type=MESH,
        )
        c.start()
        sends.append(c)

    def recv(key, ref, frm):
        k = number(key)
        pltpu.make_async_remote_copy(
            src_ref=ref, dst_ref=ref, send_sem=ssem.at[k], recv_sem=rsem.at[k],
            device_id=dev[frm], device_id_type=MESH,
        ).wait_recv()

    xf = x_ref[...].astype(f32)
    inv_x = lax.rsqrt(jnp.mean(xf * xf, axis=-1, keepdims=True) + eps)
    R[0, tp] = (xf * inv_x * pre_ref[...]).astype(bf16)
    br = br_ref[...].astype(f32)
    inv_b = lax.rsqrt(jnp.mean(br * br, axis=-1, keepdims=True) + eps)
    upst = 0.5 * oc_ref[...].astype(f32) * post_ref[...]
    R[1, tp] = (
        inv_b * upst - br * (inv_b * inv_b * inv_b) * jnp.mean(upst * br, axis=-1, keepdims=True)
    ).astype(bf16)
    own = (dw_ref, gw_ref, uw_ref)
    for m in range(3):
        W[m, zl, y] = own[m][...]

    pl.semaphore_wait(barrier, len(dev))

    def ag_own(m):
        for to in ("y+", "y-", "z+", "z-"):
            send(("o", m, to), own[m], W.at[m, zl, y], to)

    def ag_near(m):
        s = W.at[m, zl, ym]
        recv(("o", m, "y+"), s, "y-")
        a = W.at[m, zl, ym, ds(A)]
        send(("f", m, "y+"), a, a, "y+")
        for to in ("z+", "z-"):
            send(("d", m, 0, to), a, a, to)
        s = W.at[m, zl, yp]
        recv(("o", m, "y-"), s, "y+")
        b = W.at[m, zl, yp, ds(B)]
        send(("f", m, "y-"), b, b, "y-")
        a = W.at[m, zl, yp, ds(A)]
        for to in ("z+", "z-"):
            send(("d", m, 1, to), a, a, to)
        s = W.at[m, zm, y]
        recv(("o", m, "z+"), s, "z-")
        a = W.at[m, zm, y, ds(A)]
        send(("f", m, "z+"), a, a, "z+")
        b = W.at[m, zm, y, ds(B)]
        for to in ("y+", "y-"):
            send(("d", m, 0, to), b, b, to)
        s = W.at[m, zp, y]
        recv(("o", m, "z-"), s, "z+")
        b = W.at[m, zp, y, ds(B)]
        send(("f", m, "z-"), b, b, "z-")
        for to in ("y+", "y-"):
            send(("d", m, 1, to), b, b, to)

    def ag_mid(m):
        a = W.at[m, zl, y2, ds(A)]
        recv(("f", m, "y+"), a, "y-")
        for to in ("z+", "z-"):
            send(("d", m, 2, to), a, a, to)
        b = W.at[m, z2, y, ds(B)]
        recv(("f", m, "z-"), b, "z+")
        for to in ("y+", "y-"):
            send(("d", m, 2, to), b, b, to)

    def ag_diag(m, k):
        yk, zk = (ym, yp, y2)[k], (zm, zp, z2)[k]
        for frm, to, slot, q, part in (
            ("z-", "z+", (zm, yk), QA[0], A),
            ("z+", "z-", (zp, yk), QA[1], A),
            ("y-", "y+", (zk, ym), QB[0], B),
            ("y+", "y-", (zk, yp), QB[1], B),
        ):
            recv(("d", m, k, to), W.at[m, slot[0], slot[1], ds(part)], frm)
            r = W.at[m, slot[0], slot[1], ds(q)]
            send(("e", m, k, to), r, r, to)

    def ag_end(m):
        b = W.at[m, zl, y2, ds(B)]
        recv(("f", m, "y-"), b, "y+")
        a = W.at[m, z2, y, ds(A)]
        recv(("f", m, "z+"), a, "z-")
        for k in range(3):
            yk, zk = (ym, yp, y2)[k], (zm, zp, z2)[k]
            recv(("e", m, k, "z+"), W.at[m, z2, yk, ds(QA[0])], "z-")
            recv(("e", m, k, "z-"), W.at[m, z2, yk, ds(QA[1])], "z+")
            recv(("e", m, k, "y+"), W.at[m, zk, y2, ds(QB[0])], "y-")
            recv(("e", m, k, "y-"), W.at[m, zk, y2, ds(QB[1])], "y+")

    sib = 1 - core
    C = (pl.ds(0, 1024), pl.ds(1024, 1024))

    def rows_own(n):
        r = R.at[n, tp]
        for to in ("x+", "x-", "s"):
            send(("r", n, to), r, r, to)

    def rows_near(n):
        for frm, to, slot, c in (
            ("x-", "x+", xm * 2 + core, C[0]),
            ("x+", "x-", xp * 2 + core, C[1]),
        ):
            r = R.at[n, slot]
            recv(("r", n, to), r, frm)
            q = R.at[n, slot, :, c]
            send(("rf", n, to), q, q, to)
            send(("rs", n, frm), r, r, "s")

    def rows_far(n):
        slot = x2 * 2 + core
        recv(("rf", n, "x+"), R.at[n, slot, :, C[0]], "x-")
        recv(("rf", n, "x-"), R.at[n, slot, :, C[1]], "x+")
        r = R.at[n, slot]
        send(("rs", n, "2"), r, r, "s")

    def rows_end(n):
        recv(("r", n, "s"), R.at[n, x * 2 + sib], "s")
        recv(("rs", n, "x-"), R.at[n, xm * 2 + sib], "s")
        recv(("rs", n, "x+"), R.at[n, xp * 2 + sib], "s")
        recv(("rs", n, "2"), R.at[n, x2 * 2 + sib], "s")

    def factors():
        def body(i, _):
            r = pl.ds(pl.multiple_of(i * 32, 32), 32)
            g, u = gs_ref[r, :].astype(f32), us_ref[r, :].astype(f32)
            s = jax.nn.sigmoid(g)
            v = g * s
            silu[r, :] = v
            hid[r, :] = (v * u).astype(bf16)
            dgate[r, :] = u * s * (1.0 + g * (1.0 - s))
            return 0

        lax.fori_loop(0, H // 32, body, 0)

    def partial(m, left, off, n):
        def body(c, _):
            cols = pl.ds(pl.multiple_of(c * 256, 256), 256)
            right = R[n, :, :, cols].reshape(512, 256)
            out = jnp.dot(left[off : off + H, :], right, preferred_element_type=f32).astype(bf16)
            G[m, c // 2, (c % 2) * 2] = out[:, :128]
            G[m, c // 2, (c % 2) * 2 + 1] = out[:, 128:]
            return 0

        lax.fori_loop(0, 8, body, 0)

    def hidden_grad():
        def body(t, _):
            right = R[1, pl.ds(t * 4, 4)].reshape(256, 2048)
            left = jnp.concatenate([W[0, k // 4, k % 4] for k in range(16)], axis=1)
            hg = lax.dot_general(
                left, right, (((1,), (1,)), ((), ())), preferred_element_type=f32
            )
            cols = pl.ds(pl.multiple_of(t * 256, 256), 256)
            cot[pl.ds(0, H), cols] = (hg * dgate[:, cols]).astype(bf16)
            cot[pl.ds(H, H), cols] = (hg * silu[:, cols]).astype(bf16)
            return 0

        lax.fori_loop(0, 2, body, 0)

    def turn():
        for k in range(11):
            cotT[:, k * 128 : (k + 1) * 128] = cot[k * 128 : (k + 1) * 128, :].T

    def normed_grad():
        def body(c, _):
            left = cotT[...]
            zz, yy = c // 2, (c % 2) * 2
            right = jnp.concatenate(
                [
                    jnp.concatenate([W[1, zz, yy + k], W[2, zz, yy + k]], axis=0)
                    for k in range(2)
                ],
                axis=1,
            )
            out = jnp.dot(left, right, preferred_element_type=f32).astype(bf16)
            cols = pl.ds(pl.multiple_of(c * 256, 256), 256)
            NG[:, :, :, cols] = out.reshape(4, 2, 64, 256)
            return 0

        lax.fori_loop(0, 8, body, 0)

    def ng_pair():
        send("np", NG.at[:, sib], NS, "s")

    def ng_first():
        recv("np", NS, "s")

        for k in range(4):
            NG[k, core] = NG[k, core] + NS[k]
        send("n1+", NG.at[x2, core, :, C[0]], NX1.at[0], "x+")
        send("n1-", NG.at[x2, core, :, C[1]], NX1.at[1], "x-")
        send("na+", NG.at[xp, core, :, C[1]], NXa.at[0], "x+")
        send("na-", NG.at[xm, core, :, C[0]], NXa.at[1], "x-")

    def ng_second():
        recv("n1+", NX1.at[0], "x-")
        NG[xp, core, :, C[0]] = NG[xp, core, :, C[0]] + NX1[0]
        send("nb+", NG.at[xp, core, :, C[0]], NXb.at[0], "x+")
        recv("n1-", NX1.at[1], "x+")
        NG[xm, core, :, C[1]] = NG[xm, core, :, C[1]] + NX1[1]
        send("nb-", NG.at[xm, core, :, C[1]], NXb.at[1], "x-")

    def ng_end():
        recv("na+", NXa.at[0], "x-")
        recv("na-", NXa.at[1], "x+")
        recv("nb+", NXb.at[0], "x-")
        recv("nb-", NXb.at[1], "x+")
        mine = NG[x, core].astype(f32)
        h0 = mine[:, :1024] + NXb[0].astype(f32) + NXa[1].astype(f32)
        h1 = mine[:, 1024:] + NXb[1].astype(f32) + NXa[0].astype(f32)
        w = jnp.concatenate([h0, h1], axis=1) * pre_ref[...]
        xv = x_ref[...].astype(f32)
        inv = lax.rsqrt(jnp.mean(xv * xv, axis=-1, keepdims=True) + eps)
        ig_ref[...] = (
            oc_ref[...].astype(f32)
            + inv * w
            - xv * (inv * inv * inv) * jnp.mean(w * xv, axis=-1, keepdims=True)
        ).astype(bf16)

    def q(r):
        return pl.ds(QS + r[0], r[1])

    def rs_first(m):
        g = G.at[m]
        send(("a1", m, "y+"), g.at[:, y2, ds(P0)], RY1.at[m, 0], "y+")
        send(("a1", m, "y-"), g.at[:, y2, ds(P1)], RY1.at[m, 1], "y-")
        send(("b1", m, "z+"), g.at[z2, :, q(Q0)], RZ1.at[m, 0], "z+")
        send(("b1", m, "z-"), g.at[z2, :, q(Q1)], RZ1.at[m, 1], "z-")
        send(("aa", m, "y+"), g.at[:, yp, ds(P1)], RYa.at[m, 0], "y+")
        send(("aa", m, "y-"), g.at[:, ym, ds(P0)], RYa.at[m, 1], "y-")
        send(("ba", m, "z+"), g.at[zp, :, q(Q1)], RZa.at[m, 0], "z+")
        send(("ba", m, "z-"), g.at[zm, :, q(Q0)], RZa.at[m, 1], "z-")

    def rs_second(m):
        g = G.at[m]
        recv(("b1", m, "z+"), RZ1.at[m, 0], "z-")
        G[m, zp, :, q(Q0)] = G[m, zp, :, q(Q0)] + RZ1[m, 0]
        send(("bb", m, "z+"), g.at[zp, :, q(Q0)], RZb.at[m, 0], "z+")
        recv(("b1", m, "z-"), RZ1.at[m, 1], "z+")
        G[m, zm, :, q(Q1)] = G[m, zm, :, q(Q1)] + RZ1[m, 1]
        send(("bb", m, "z-"), g.at[zm, :, q(Q1)], RZb.at[m, 1], "z-")
        recv(("a1", m, "y+"), RY1.at[m, 0], "y-")
        G[m, :, yp, ds(P0)] = G[m, :, yp, ds(P0)] + RY1[m, 0]
        send(("ab", m, "y+"), g.at[:, yp, ds(P0)], RYb.at[m, 0], "y+")
        recv(("a1", m, "y-"), RY1.at[m, 1], "y+")
        G[m, :, ym, ds(P1)] = G[m, :, ym, ds(P1)] + RY1[m, 1]
        send(("ab", m, "y-"), g.at[:, ym, ds(P1)], RYb.at[m, 1], "y-")

    def add3(a, b, c):
        return (a.astype(f32) + b.astype(f32) + c.astype(f32)).astype(bf16)

    def rs_third(m):
        g = G.at[m]
        recv(("ba", m, "z+"), RZa.at[m, 0], "z-")
        recv(("ba", m, "z-"), RZa.at[m, 1], "z+")
        recv(("bb", m, "z+"), RZb.at[m, 0], "z-")
        recv(("bb", m, "z-"), RZb.at[m, 1], "z+")
        G[m, zl, :, q(Q0)] = add3(G[m, zl, :, q(Q0)], RZb[m, 0], RZa[m, 1])
        G[m, zl, :, q(Q1)] = add3(G[m, zl, :, q(Q1)], RZb[m, 1], RZa[m, 0])
        send(("c1", m, "y+"), g.at[zl, y2, q(Q0)], SY1.at[m, 0], "y+")
        send(("c1", m, "y-"), g.at[zl, y2, q(Q1)], SY1.at[m, 1], "y-")
        send(("ca", m, "y+"), g.at[zl, yp, q(Q1)], SYa.at[m, 0], "y+")
        send(("ca", m, "y-"), g.at[zl, ym, q(Q0)], SYa.at[m, 1], "y-")
        recv(("aa", m, "y+"), RYa.at[m, 0], "y-")
        recv(("aa", m, "y-"), RYa.at[m, 1], "y+")
        recv(("ab", m, "y+"), RYb.at[m, 0], "y-")
        recv(("ab", m, "y-"), RYb.at[m, 1], "y+")
        G[m, :, y, ds(P0)] = add3(G[m, :, y, ds(P0)], RYb[m, 0], RYa[m, 1])
        G[m, :, y, ds(P1)] = add3(G[m, :, y, ds(P1)], RYb[m, 1], RYa[m, 0])
        send(("d1", m, "z+"), g.at[z2, y, ds(P0)], SZ1.at[m, 0], "z+")
        send(("d1", m, "z-"), g.at[z2, y, ds(P1)], SZ1.at[m, 1], "z-")
        send(("da", m, "z+"), g.at[zp, y, ds(P1)], SZa.at[m, 0], "z+")
        send(("da", m, "z-"), g.at[zm, y, ds(P0)], SZa.at[m, 1], "z-")

    def rs_fourth(m):
        g = G.at[m]
        recv(("c1", m, "y+"), SY1.at[m, 0], "y-")
        G[m, zl, yp, q(Q0)] = G[m, zl, yp, q(Q0)] + SY1[m, 0]
        send(("cb", m, "y+"), g.at[zl, yp, q(Q0)], SYb.at[m, 0], "y+")
        recv(("c1", m, "y-"), SY1.at[m, 1], "y+")
        G[m, zl, ym, q(Q1)] = G[m, zl, ym, q(Q1)] + SY1[m, 1]
        send(("cb", m, "y-"), g.at[zl, ym, q(Q1)], SYb.at[m, 1], "y-")
        recv(("d1", m, "z+"), SZ1.at[m, 0], "z-")
        G[m, zp, y, ds(P0)] = G[m, zp, y, ds(P0)] + SZ1[m, 0]
        send(("db", m, "z+"), g.at[zp, y, ds(P0)], SZb.at[m, 0], "z+")
        recv(("d1", m, "z-"), SZ1.at[m, 1], "z+")
        G[m, zm, y, ds(P1)] = G[m, zm, y, ds(P1)] + SZ1[m, 1]
        send(("db", m, "z-"), g.at[zm, y, ds(P1)], SZb.at[m, 1], "z-")

    X0, X1 = pl.ds(0, 352), pl.ds(352, 352)

    def rs_fifth(m):
        recv(("ca", m, "y+"), SYa.at[m, 0], "y-")
        recv(("ca", m, "y-"), SYa.at[m, 1], "y+")
        recv(("cb", m, "y+"), SYb.at[m, 0], "y-")
        recv(("cb", m, "y-"), SYb.at[m, 1], "y+")
        T[m, q(Q0)] = add3(G[m, zl, y, q(Q0)], SYb[m, 0], SYa[m, 1])
        T[m, q(Q1)] = add3(G[m, zl, y, q(Q1)], SYb[m, 1], SYa[m, 0])
        recv(("da", m, "z+"), SZa.at[m, 0], "z-")
        recv(("da", m, "z-"), SZa.at[m, 1], "z+")
        recv(("db", m, "z+"), SZb.at[m, 0], "z-")
        recv(("db", m, "z-"), SZb.at[m, 1], "z+")
        T[m, ds(P0)] = add3(G[m, zl, y, ds(P0)], SZb[m, 0], SZa[m, 1])
        T[m, ds(P1)] = add3(G[m, zl, y, ds(P1)], SZb[m, 1], SZa[m, 0])
        send(("x", m, "zz+"), T.at[m, X0], XF.at[m, 0], "zz+")
        send(("x", m, "zz-"), T.at[m, X1], XF.at[m, 1], "zz-")

    def rs_sixth(m):
        recv(("x", m, "zz+"), XF.at[m, 0], "zz-")
        send(("xf", m, "zz+"), XF.at[m, 0], XR.at[m, X0], "zz+")
        recv(("x", m, "zz-"), XF.at[m, 1], "zz+")
        send(("xf", m, "zz-"), XF.at[m, 1], XR.at[m, X1], "zz-")

    outs = (dg_ref, gg_ref, ug_ref)

    def rs_end(m):
        recv(("xf", m, "zz+"), XR.at[m, X0], "zz-")
        recv(("xf", m, "zz-"), XR.at[m, X1], "zz+")
        outs[m][...] = T[m].astype(f32) + XR[m].astype(f32)

    ag_own(0)
    rows_own(1)
    rows_own(0)
    ag_own(1)
    factors()
    ag_near(0)
    ag_own(2)
    rows_near(1)
    ag_near(1)
    rows_near(0)
    ag_mid(0)
    ag_near(2)
    ag_diag(0, 0)
    ag_diag(0, 1)
    rows_far(1)
    ag_mid(1)
    rows_far(0)
    ag_diag(0, 2)
    rows_end(1)
    partial(0, hid, 0, 1)
    rs_first(0)
    ag_mid(2)
    ag_diag(1, 0)
    ag_diag(1, 1)
    ag_end(0)
    hidden_grad()
    rows_end(0)
    partial(1, cot, 0, 0)
    rs_first(1)
    ag_diag(1, 2)
    ag_diag(2, 0)
    ag_diag(2, 1)
    partial(2, cot, H, 0)
    rs_first(2)
    ag_diag(2, 2)
    rs_second(0)
    turn()
    ag_end(1)
    ag_end(2)
    normed_grad()
    ng_pair()
    rs_third(0)
    rs_second(1)
    ng_first()
    rs_fourth(0)
    ng_second()
    rs_second(2)
    rs_third(1)
    rs_fifth(0)
    rs_fourth(1)
    ng_end()
    rs_sixth(0)
    rs_third(2)
    rs_fifth(1)
    rs_fourth(2)
    rs_sixth(1)
    rs_end(0)
    rs_fifth(2)
    rs_end(1)
    rs_sixth(2)
    rs_end(2)
    for c in sends:
        c.wait_send()


def per_device(x, pre, post, gs, us, br, oc, gw, uw, dw):
    vmem = pl.BlockSpec(memory_space=pltpu.VMEM)
    V = pltpu.VMEM
    sds = jax.ShapeDtypeStruct
    ig, gg, ug, dg = pl.pallas_call(
        kernel,
        out_shape=(
            sds((64, 2048), bf16), sds((H, 128), f32), sds((H, 128), f32), sds((H, 128), f32),
        ),
        in_specs=[vmem] * 10,
        out_specs=(vmem,) * 4,
        scratch_shapes=[
            V((3, 4, 4, H, 128), bf16),
            V((2, 8, 64, 2048), bf16),
            V((3, 4, 4, H, 128), bf16),
            V((3, 2, 4, 256, 128), bf16),
            V((3, 2, 4, 256, 128), bf16),
            V((3, 2, 4, 256, 128), bf16),
            V((3, 2, 4, 96, 128), bf16),
            V((3, 2, 4, 96, 128), bf16),
            V((3, 2, 4, 96, 128), bf16),
            V((3, 2, 96, 128), bf16),
            V((3, 2, 96, 128), bf16),
            V((3, 2, 96, 128), bf16),
            V((3, 2, 256, 128), bf16),
            V((3, 2, 256, 128), bf16),
            V((3, 2, 256, 128), bf16),
            V((3, H, 128), bf16),
            V((3, 2, 352, 128), bf16),
            V((3, H, 128), bf16),
            V((H, 512), f32),
            V((H, 512), f32),
            V((H, 512), bf16),
            V((2 * H, 512), bf16),
            V((512, 2 * H), bf16),
            V((4, 2, 64, 2048), bf16),
            V((4, 64, 2048), bf16),
            V((2, 64, 1024), bf16),
            V((2, 64, 1024), bf16),
            V((2, 64, 1024), bf16),
            pltpu.SemaphoreType.DMA((N_SEM,)),
            pltpu.SemaphoreType.DMA((N_SEM,)),
        ],
        compiler_params=pltpu.CompilerParams(
            collective_id=0, has_side_effects=True, vmem_limit_bytes=66 * 1000 * 1000
        ),
        name="ffn_backward",
    )(x, pre.reshape(1, -1), post.reshape(1, -1), gs.T, us.T, br, oc, gw.T, uw.T, dw.T)
    return ig, gg.T, ug.T, dg.T


def solution(mesh):
    return jax.shard_map(
        per_device,
        mesh=mesh,
        in_specs=(
            P(("rep", "fs", "tp"), None),
            P(),
            P(),
            P(("rep", "fs"), "tp"),
            P(("rep", "fs"), "tp"),
            P(("rep", "fs", "tp"), None),
            P(("rep", "fs", "tp"), None),
            P("fs", "tp"),
            P("fs", "tp"),
            P("fs", "tp"),
        ),
        out_specs=(P(("rep", "fs", "tp"), None), P("fs", "tp"), P("fs", "tp"), P("fs", "tp")),
        check_vma=False,
    )
```

```python
import jax
import jax.numpy as jnp
from jax import lax
from jax.experimental import pallas as pl
from jax.experimental.pallas import tpu as pltpu
from jax.sharding import PartitionSpec as P

MESH = pl.DeviceIdType.MESH
bf16, f32 = jnp.bfloat16, jnp.float32
eps = 1e-06

H = 704
NA = (576, 32, 416)
NP = (384, 416, 448)
N_RECV, N_SEND, N_LOCAL = 160, 48, 32
ORDER = (
    2, 51, 3, 85, 27, 0, 80, 1, 75, 81, 82, 19, 9, 10, 4, 5, 14, 15, 20, 33, 43, 38, 28, 76, 77, 25,
    11, 12, 57, 58, 62, 52, 53, 67, 68, 63, 24, 17, 83, 6, 22, 7, 84, 86, 78, 8, 99, 21, 98, 16, 13,
    72, 79, 55, 60, 54, 65, 59, 70, 102, 103, 105, 106, 108, 69, 109, 111, 44, 39, 29, 34, 49, 48,
    112, 64, 73, 18, 23, 101, 104, 113, 120, 107, 36, 31, 66, 71, 35, 40, 30, 41, 42, 45, 46, 47,
    37, 26, 87, 122, 110, 32, 115, 88, 61, 129, 56, 89, 158, 100, 90, 159, 116, 50, 123, 74, 91,
    163, 162, 92, 166, 168, 93, 169, 165, 171, 172, 95, 173, 180, 94, 114, 121, 96, 161, 128, 117,
    124, 164, 167, 160, 170, 175, 118, 182, 125, 97, 132, 143, 150, 133, 135, 136, 138, 139, 176,
    141, 183, 142, 119, 126, 130, 174, 181, 131, 177, 184, 134, 137, 127, 140, 145, 152, 144, 151,
    178, 185, 148, 155, 146, 153, 179, 186, 149, 156, 147, 154, 187, 157,
)


def halves(lo, hi):
    n = (hi - lo) // 2
    return (lo, hi - lo), (lo, n), (lo + n, n)


GA = [halves(0, n) for n in NA]
GB = [halves(n, H) for n in NA]
SP = [halves(0, n) for n in NP]
SQ = [halves(n, H) for n in NP]


def ds(r):
    return pl.ds(r[0], r[1])


def mod(a, n):
    return lax.rem(a + n, n)


def kernel(
    x_hbm, pre_hbm, post_hbm, gs_hbm, us_hbm, br_hbm, oc_hbm, gw_ref, uw_ref, dw_ref,
    ig_hbm, d_my, g_my, u_my, d_th, g_th, u_th,
    *scratch,
):
    s = dict(zip(SCRATCH, scratch))
    W, R, G, T, XF = s["W"], s["R"], s["G"], s["T"], s["XF"]
    silu, dgate, hid, cot, cotT = s["silu"], s["dgate"], s["hid"], s["cot"], s["cotT"]
    NG, NS, NX1, NXc = s["NG"], s["NS"], s["NX1"], s["NXc"]
    x_ref, pre_ref, post_ref, br_ref, oc_ref = s["x"], s["pre"], s["post"], s["br"], s["oc"]
    gs_ref, us_ref, ig_ref = s["gs"], s["us"], s["ig"]
    mine, theirs = (d_my, g_my, u_my), (d_th, g_th, u_th)
    ssem, rsem, lsem = s["ssem"], s["rsem"], s["lsem"]
    RY1, RYc, RZ1, RZc, SY1, SYc, SZ1, SZc = (
        [s[n + k + str(m)] for m in range(3)] for n in ("RY", "RZ", "SY", "SZ") for k in "1c"
    )
    rep, fs, tp = lax.axis_index("rep"), lax.axis_index("fs"), lax.axis_index("tp")
    zl, y = fs // 4, fs % 4
    z = rep * 4 + zl
    x, core = tp // 2, tp % 2
    ym, yp, y2 = mod(y - 1, 4), mod(y + 1, 4), mod(y + 2, 4)
    zm, zp, z2 = mod(zl - 1, 4), mod(zl + 1, 4), mod(zl + 2, 4)
    xm, xp, x2 = mod(x - 1, 4), mod(x + 1, 4), mod(x + 2, 4)

    def zdev(d):
        zz = mod(z + d, 8)
        return {"rep": zz // 4, "fs": (zz % 4) * 4 + y}

    dev = {
        "y+": {"fs": zl * 4 + yp},
        "y-": {"fs": zl * 4 + ym},
        "z+": zdev(1),
        "z-": zdev(-1),
        "zz+": zdev(2),
        "zz-": zdev(-2),
        "x+": {"tp": xp * 2 + core},
        "x-": {"tp": xm * 2 + core},
        "s": {"tp": x * 2 + 1 - core},
    }

    barrier = pltpu.get_barrier_semaphore()
    for name in dev:
        pl.semaphore_signal(barrier, inc=1, device_id=dev[name], device_id_type=MESH)

    ids = {}
    sends = []
    count = [0]

    def number(key):
        return ids.setdefault(key, len(ids))

    def send(key, src, dst, to):
        if 0 in src.shape:
            return
        if len(sends) == N_SEND:
            sends.pop(0).wait_send()
        c = pltpu.make_async_remote_copy(
            src_ref=src, dst_ref=dst, send_sem=ssem.at[count[0] % N_SEND],
            recv_sem=rsem.at[number(key)], device_id=dev[to], device_id_type=MESH,
        )
        c.start()
        count[0] += 1
        sends.append(c)

    def recv(key, ref):
        if 0 in ref.shape:
            return
        k = number(key)
        pltpu.make_async_copy(ref, ref, rsem.at[k]).wait()

    own = (dw_ref, gw_ref, uw_ref)
    local = {}

    def load(key, src, dst):
        c = pltpu.make_async_copy(src, dst, lsem.at[len(local)])
        c.start()
        local[key] = c

    load("br", br_hbm, br_ref)
    load("oc", oc_hbm, oc_ref)
    load("post", post_hbm, post_ref)
    load("x", x_hbm, x_ref)
    load("pre", pre_hbm, pre_ref)
    load("gs", gs_hbm, gs_ref)
    load("us", us_hbm, us_ref)
    for m in range(3):
        load(("w", m), own[m], W.at[m, zl, y])

    def rows_b():
        for key in ("br", "oc", "post"):
            local[key].wait()
        br = br_ref[...].astype(f32)
        inv_b = lax.rsqrt(jnp.mean(br * br, axis=-1, keepdims=True) + eps)
        upst = 0.5 * oc_ref[...].astype(f32) * post_ref[...]
        mean = jnp.mean(upst * br, axis=-1, keepdims=True)
        R[1, tp] = (inv_b * upst - br * (inv_b * inv_b * inv_b) * mean).astype(bf16)

    def rows_n():
        for key in ("x", "pre"):
            local[key].wait()
        xf = x_ref[...].astype(f32)
        inv_x = lax.rsqrt(jnp.mean(xf * xf, axis=-1, keepdims=True) + eps)
        R[0, tp] = (xf * inv_x * pre_ref[...]).astype(bf16)

    ev = [rows_b, rows_n]

    def event(fn, *args):
        ev.append(lambda: fn(*args))

    def enter():
        pl.semaphore_wait(barrier, len(dev))

    event(enter)

    AXES = ("y+", "y-", "z+", "z-")
    NEAR = ((zl, ym), (zl, yp), (zm, y), (zp, y))

    def ag_own(m):
        for to in ("y+", "y-", "z+", "z-"):
            send(("o", m, to), own[m], W.at[m, zl, y], to)

    def ag_forward(m, d):
        to = AXES[d]
        zz, yy = NEAR[d]
        recv(("o", m, to), W.at[m, zz, yy])
        part = W.at[m, zz, yy, ds((GA, GB)[d % 2][m][0])]
        send(("f", m, to) if d in (0, 3) else ("w", m), part, part, to)

    def ag_turn(m, d):
        zz, yy = NEAR[d]
        part = W.at[m, zz, yy, ds((GA, GB)[d // 2][m][0])]
        for to in (("z+", "z-"), ("y+", "y-"))[d // 2]:
            send(("d", m, d % 2, to), part, part, to)

    def ag_mid(m, axis):
        if axis == 0:
            part = W.at[m, zl, y2, ds(GA[m][0])]
            recv(("f", m, "y+"), part)
        else:
            part = W.at[m, z2, y, ds(GB[m][0])]
            recv(("f", m, "z-"), part)
        for to in (("z+", "z-"), ("y+", "y-"))[axis]:
            send(("d", m, 2, to), part, part, to)

    def ag_diag(m, k, d):
        to = AXES[d]
        yk, zk = (ym, yp, y2)[k], (zm, zp, z2)[k]
        zz, yy = ((zk, ym), (zk, yp), (zm, yk), (zp, yk))[d]
        g = (GB, GA)[d // 2][m]
        recv(("d", m, k, to), W.at[m, zz, yy, ds(g[0])])
        part = W.at[m, zz, yy, ds(g[1 + d % 2])]
        send(("w", m), part, part, to)

    def ag_end(m):
        local[("w", m)].wait()
        recv(("w", m), W.at[m, 0])

    for m in range(3):
        event(ag_own, m)
        for d in range(4):
            event(ag_forward, m, d)
            event(ag_turn, m, d)
            for k in range(3):
                event(ag_diag, m, k, d)
        for axis in range(2):
            event(ag_mid, m, axis)
        event(ag_end, m)

    sib = 1 - core
    C = (pl.ds(0, 1024), pl.ds(1024, 1024))
    XS = (("x+", xm), ("x-", xp))

    def rows_own(n):
        r = R.at[n, tp]
        for to in ("x+", "x-", "s"):
            send(("r", n, to) if to != "s" else ("j", n), r, r, to)

    def rows_near(n, d):
        to, xx = XS[d]
        r = R.at[n, xx * 2 + core]
        recv(("r", n, to), r)
        part = R.at[n, xx * 2 + core, :, C[d]]
        send(("rf", n), part, part, to)
        send(("j", n), r, r, "s")

    def rows_far(n):
        r = R.at[n, x2 * 2 + core]
        recv(("rf", n), r)
        send(("j", n), r, r, "s")

    def rows_end(n):
        recv(("j", n), R.at[n, pl.ds(0, 4)])

    for n in range(2):
        event(rows_own, n)
        for d in range(2):
            event(rows_near, n, d)
        event(rows_far, n)
        event(rows_end, n)

    def factors():
        local["gs"].wait()
        local["us"].wait()

        def body(i, _):
            r = pl.ds(pl.multiple_of(i * 32, 32), 32)
            g, u = gs_ref[r, :].astype(f32), us_ref[r, :].astype(f32)
            s = jax.nn.sigmoid(g)
            v = g * s
            silu[r, :] = v
            hid[r, :] = (v * u).astype(bf16)
            dgate[r, :] = u * s * (1.0 + g * (1.0 - s))
            return 0

        lax.fori_loop(0, H // 32, body, 0)

    def partial(m, left, off, n):
        def body(c, _):
            cols = pl.ds(pl.multiple_of(c * 512, 512), 512)
            right = R[n, :, :, cols].reshape(512, 512)
            out = jnp.dot(left[off : off + H, :], right, preferred_element_type=f32).astype(bf16)
            for k in range(4):
                G[m, c, k] = out[:, k * 128 : (k + 1) * 128]
            return 0

        lax.fori_loop(0, 4, body, 0)

    def hidden_grad():
        def body(t, _):
            right = R[1, pl.ds(t * 4, 4)].reshape(256, 2048)
            left = jnp.concatenate([W[0, k // 4, k % 4] for k in range(16)], axis=1)
            hg = lax.dot_general(
                left, right, (((1,), (1,)), ((), ())), preferred_element_type=f32
            )
            cols = pl.ds(pl.multiple_of(t * 256, 256), 256)
            cot[pl.ds(0, H), cols] = (hg * dgate[:, cols]).astype(bf16)
            cot[pl.ds(H, H), cols] = (hg * silu[:, cols]).astype(bf16)
            return 0

        lax.fori_loop(0, 2, body, 0)

    def turn():
        for k in range(11):
            cotT[:, k * 128 : (k + 1) * 128] = cot[k * 128 : (k + 1) * 128, :].T

    def normed_grad(h):
        def body(c, _):
            right = jnp.concatenate(
                [jnp.concatenate([W[1, c, k], W[2, c, k]], axis=0) for k in range(4)], axis=1
            )
            out = jnp.dot(cotT[...], right, preferred_element_type=f32).astype(bf16)
            cols = pl.ds(pl.multiple_of(c * 512, 512), 512)
            NG[:, :, :, cols] = out.reshape(4, 2, 64, 512)
            return 0

        lax.fori_loop(2 * h, 2 * h + 2, body, 0)
        send(("np", h), NG.at[:, sib, :, C[h]], NS.at[:, :, C[h]], "s")

    event(factors)
    event(partial, 0, hid, 0, 1)
    event(hidden_grad)
    event(partial, 1, cot, 0, 0)
    event(partial, 2, cot, H, 0)
    event(turn)
    event(normed_grad, 0)
    event(normed_grad, 1)

    def ng_first(h):
        recv(("np", h), NS.at[:, :, C[h]])
        for k in range(4):
            NG[k, core, :, C[h]] = NG[k, core, :, C[h]] + NS[k, :, C[h]]
        to, back = (("x+", "x-"), ("x-", "x+"))[h]
        send(("n1", h), NG.at[x2, core, :, C[h]], NX1.at[h], to)
        send("n", NG.at[(xm, xp)[h], core, :, C[h]], NXc.at[2 + h], back)

    def ng_second(h):
        to, nxt = (("x+", xp), ("x-", xm))[h]
        recv(("n1", h), NX1.at[h])
        NG[nxt, core, :, C[h]] = NG[nxt, core, :, C[h]] + NX1[h]
        send("n", NG.at[nxt, core, :, C[h]], NXc.at[h], to)

    def ng_end():
        w = []
        recv("n", NXc)
        for h in range(2):
            w.append(
                NG[x, core, :, C[h]].astype(f32) + NXc[h].astype(f32) + NXc[2 + h].astype(f32)
            )
        w = jnp.concatenate(w, axis=1) * pre_ref[...]
        xv = x_ref[...].astype(f32)
        inv = lax.rsqrt(jnp.mean(xv * xv, axis=-1, keepdims=True) + eps)
        ig_ref[...] = (
            oc_ref[...].astype(f32)
            + inv * w
            - xv * (inv * inv * inv) * jnp.mean(w * xv, axis=-1, keepdims=True)
        ).astype(bf16)
        load("ig", ig_ref, ig_hbm)

    for h in range(2):
        event(ng_first, h)
        event(ng_second, h)
    event(ng_end)

    CH = (z2, zp, zm, zl)

    def rs_first_y(m):
        for c in range(4):
            for d, to in ((0, "y+"), (1, "y-")):
                src = G.at[m, CH[c], y2, ds(SP[m][1 + d])]
                send(("a1", m, c, d), src, RY1[m].at[d, c], to)
        for c in range(4):
            for d, to in ((0, "y+"), (1, "y-")):
                src = G.at[m, CH[c], (yp, ym)[d], ds(SP[m][2 - d])]
                send(("C", m, c), src, RYc[m].at[c, 2 + d], to)

    def rs_first_z(m):
        for d, to in ((0, "z+"), (1, "z-")):
            send(("b1", m, d), G.at[m, z2, :, ds(SQ[m][1 + d])], RZ1[m].at[d], to)
        for d, to in ((0, "z+"), (1, "z-")):
            src = G.at[m, (zp, zm)[d], :, ds(SQ[m][2 - d])]
            send(("D", m), src, RZc[m].at[2 + d], to)

    def rs_second_y(m, c, d):
        to, nxt = (("y+", yp), ("y-", ym))[d]
        r = ds(SP[m][1 + d])
        recv(("a1", m, c, d), RY1[m].at[d, c])
        G[m, CH[c], nxt, r] = G[m, CH[c], nxt, r] + RY1[m][d, c]
        send(("C", m, c), G.at[m, CH[c], nxt, r], RYc[m].at[c, d], to)

    def rs_second_z(m, d):
        to, nxt = (("z+", zp), ("z-", zm))[d]
        r = ds(SQ[m][1 + d])
        recv(("b1", m, d), RZ1[m].at[d])
        G[m, nxt, :, r] = G[m, nxt, :, r] + RZ1[m][d]
        send(("D", m), G.at[m, nxt, :, r], RZc[m].at[d], to)

    def add3(a, b, c):
        return (a.astype(f32) + b.astype(f32) + c.astype(f32)).astype(bf16)

    def rs_third_y(m, c):
        recv(("C", m, c), RYc[m].at[c])
        for d in range(2):
            r = ds(SP[m][1 + d])
            G[m, CH[c], y, r] = add3(G[m, CH[c], y, r], RYc[m][c, d], RYc[m][c, 3 - d])
        if c == 0:
            for d, to in ((0, "z+"), (1, "z-")):
                send(("d1", m, d), G.at[m, z2, y, ds(SP[m][1 + d])], SZ1[m].at[d], to)
        elif c < 3:
            d, to = c - 1, ("z+", "z-")[c - 1]
            send(("T", m, 0, 1 - d), G.at[m, CH[c], y, ds(SP[m][2 - d])], SZc[m].at[1 - d, 1], to)

    def rs_third_z(m):
        recv(("D", m), RZc[m])
        for d in range(2):
            r = ds(SQ[m][1 + d])
            if r.size:
                G[m, zl, :, r] = add3(G[m, zl, :, r], RZc[m][d], RZc[m][3 - d])
        for d, to in ((0, "y+"), (1, "y-")):
            send(("c1", m, d), G.at[m, zl, y2, ds(SQ[m][1 + d])], SY1[m].at[d], to)
        for d, to in ((0, "y+"), (1, "y-")):
            src = G.at[m, zl, (yp, ym)[d], ds(SQ[m][2 - d])]
            send(("T", m, 1, 1 - d), src, SYc[m].at[1 - d, 1], to)

    def rs_fourth_y(m, d):
        to, nxt = (("y+", yp), ("y-", ym))[d]
        r = ds(SQ[m][1 + d])
        recv(("c1", m, d), SY1[m].at[d])
        G[m, zl, nxt, r] = G[m, zl, nxt, r] + SY1[m][d]
        send(("T", m, 1, d), G.at[m, zl, nxt, r], SYc[m].at[d, 0], to)

    def rs_fourth_z(m, d):
        to, nxt = (("z+", zp), ("z-", zm))[d]
        r = ds(SP[m][1 + d])
        recv(("d1", m, d), SZ1[m].at[d])
        G[m, nxt, y, r] = G[m, nxt, y, r] + SZ1[m][d]
        send(("T", m, 0, d), G.at[m, nxt, y, r], SZc[m].at[d, 0], to)

    def rs_fifth(m, k, d):
        r = ds((SP, SQ)[k][m][1 + d])
        if not r.size:
            return
        c = (SZc, SYc)[k][m]
        recv(("T", m, k, d), c.at[d])
        T[m, r] = add3(G[m, zl, y, r], c[d, 0], c[d, 1])
        send(("x", m, k, d), T.at[m, r], XF.at[m, r], ("zz+", "zz-")[d])
        load(("out", m, k, d), T.at[m, r], mine[m].at[r])

    def rs_sixth(m, k, d):
        r = ds((SP, SQ)[k][m][1 + d])
        recv(("x", m, k, d), XF.at[m, r])
        send(("z", m), XF.at[m, r], theirs[m].at[r], ("zz+", "zz-")[d])

    def rs_end(m):
        recv(("z", m), theirs[m])

    for m in range(3):
        event(rs_first_y, m)
        event(rs_first_z, m)
        event(rs_third_z, m)
        for c in range(4):
            event(rs_third_y, m, c)
            for d in range(2):
                event(rs_second_y, m, c, d)
        for d in range(2):
            event(rs_second_z, m, d)
            event(rs_fourth_y, m, d)
            event(rs_fourth_z, m, d)
            for k in range(2):
                event(rs_fifth, m, k, d)
                event(rs_sixth, m, k, d)
        event(rs_end, m)

    for k in ORDER:
        ev[k]()
    assert len(ORDER) == len(ev) and len(ids) <= N_RECV
    for c in sends:
        c.wait_send()
    for key in local:
        if key == "ig" or key[0] == "out":
            local[key].wait()


V, SEM = pltpu.VMEM, pltpu.SemaphoreType.DMA
SCRATCH = {
    "W": V((3, 4, 4, H, 128), bf16),
    "R": V((2, 8, 64, 2048), bf16),
    "G": V((3, 4, 4, H, 128), bf16),
    "T": V((3, H, 128), bf16),
    "XF": V((3, H, 128), bf16),
    "silu": V((H, 512), f32),
    "dgate": V((H, 512), f32),
    "hid": V((H, 512), bf16),
    "cot": V((2 * H, 512), bf16),
    "cotT": V((512, 2 * H), bf16),
    "NG": V((4, 2, 64, 2048), bf16),
    "NS": V((4, 64, 2048), bf16),
    "NX1": V((2, 64, 1024), bf16),
    "NXc": V((4, 64, 1024), bf16),
    "x": V((64, 2048), bf16),
    "br": V((64, 2048), bf16),
    "oc": V((64, 2048), bf16),
    "pre": V((1, 2048), f32),
    "post": V((1, 2048), f32),
    "gs": V((H, 512), bf16),
    "us": V((H, 512), bf16),
    "ig": V((64, 2048), bf16),
    "ssem": SEM((N_SEND,)),
    "rsem": SEM((N_RECV,)),
    "lsem": SEM((N_LOCAL,)),
}
for m in range(3):
    p, q = SP[m][1][1], SQ[m][1][1]
    SCRATCH["RY1" + str(m)] = V((2, 4, p, 128), bf16)
    SCRATCH["RYc" + str(m)] = V((4, 4, p, 128), bf16)
    SCRATCH["RZ1" + str(m)] = V((2, 4, max(q, 16), 128), bf16)
    SCRATCH["RZc" + str(m)] = V((4, 4, max(q, 16), 128), bf16)
    SCRATCH["SZ1" + str(m)] = V((2, p, 128), bf16)
    SCRATCH["SZc" + str(m)] = V((2, 2, p, 128), bf16)
    SCRATCH["SY1" + str(m)] = V((2, max(q, 16), 128), bf16)
    SCRATCH["SYc" + str(m)] = V((2, 2, max(q, 16), 128), bf16)


def finish(ig, *refs):
    parts, (ig_out, *outs), (row, both, total, sem) = refs[:6], refs[6:10], refs[10:]
    load = [
        pltpu.make_async_copy(src, both.at[k], sem.at[k]) for k, src in enumerate(parts)
    ]
    load.append(pltpu.make_async_copy(ig, row, sem.at[6]))
    for c in load:
        c.start()
    store = [pltpu.make_async_copy(row, ig_out, sem.at[10])]
    for m in range(3):
        load[m].wait()
        load[3 + m].wait()
        total[m] = both[m].astype(f32) + both[3 + m].astype(f32)
        store.append(pltpu.make_async_copy(total.at[m], outs[m], sem.at[7 + m]))
        store[-1].start()
    load[6].wait()
    store[0].start()
    for c in store:
        c.wait()


def per_device(x, pre, post, gs, us, br, oc, gw, uw, dw):
    hbm = pl.BlockSpec(memory_space=pl.ANY)
    sds = jax.ShapeDtypeStruct
    ig, *pairs = pl.pallas_call(
        kernel,
        out_shape=(sds((64, 2048), bf16), *[sds((H, 128), bf16) for _ in range(6)]),
        in_specs=[hbm] * 10,
        out_specs=(hbm,) * 7,
        scratch_shapes=list(SCRATCH.values()),
        compiler_params=pltpu.CompilerParams(
            collective_id=0, has_side_effects=True, vmem_limit_bytes=67_000_000
        ),
        name="ffn_backward",
    )(x, pre.reshape(1, -1), post.reshape(1, -1), gs.T, us.T, br, oc, gw.T, uw.T, dw.T)
    ig, dg, gg, ug = pl.pallas_call(
        finish,
        out_shape=(sds((64, 2048), bf16), *[sds((H, 128), f32) for _ in range(3)]),
        in_specs=[hbm] * 7,
        out_specs=(hbm,) * 4,
        scratch_shapes=[
            V((64, 2048), bf16), V((6, H, 128), bf16), V((3, H, 128), f32), SEM((11,)),
        ],
        name="finish",
    )(ig, *pairs)
    return ig, gg.T, ug.T, dg.T


def solution(mesh):
    return jax.shard_map(
        per_device,
        mesh=mesh,
        in_specs=(
            P(("rep", "fs", "tp"), None),
            P(),
            P(),
            P(("rep", "fs"), "tp"),
            P(("rep", "fs"), "tp"),
            P(("rep", "fs", "tp"), None),
            P(("rep", "fs", "tp"), None),
            P("fs", "tp"),
            P("fs", "tp"),
            P("fs", "tp"),
        ),
        out_specs=(P(("rep", "fs", "tp"), None), P("fs", "tp"), P("fs", "tp"), P("fs", "tp")),
        check_vma=False,
    )
```

```python
import jax
import jax.numpy as jnp
from jax import lax
from jax.experimental import pallas as pl
from jax.experimental.pallas import tpu as pltpu
from jax.sharding import PartitionSpec as P

MESH = pl.DeviceIdType.MESH
bf16, f32 = jnp.bfloat16, jnp.float32
eps = 1e-06

HU = 352
QU = HU // 2
NQ = (192, 192, 128)
N_RECV, N_SEND, N_LOCAL = 108, 48, 20
ORDER = (
    2, 12, 0, 38, 1, 30, 47, 21, 13, 16, 14, 22, 3, 25, 40, 17, 15, 46, 39, 4, 26, 32, 18, 7, 31,
    41, 23, 42, 19, 5, 8, 24, 43, 6, 33, 27, 34, 9, 35, 28, 44, 10, 48, 45, 49, 62, 76, 11, 36, 50,
    37, 52, 122, 65, 77, 108, 63, 51, 69, 67, 85, 99, 29, 53, 123, 66, 20, 55, 64, 78, 70, 100, 68,
    111, 124, 58, 71, 113, 54, 115, 112, 109, 101, 56, 114, 125, 72, 116, 86, 110, 59, 88, 102, 90,
    92, 126, 87, 73, 117, 89, 91, 93, 79, 57, 103, 127, 94, 74, 118, 128, 104, 80, 95, 105, 75, 81,
    119, 60, 129, 96, 82, 120, 97, 106, 83, 61, 121, 98, 84, 130, 107,
)


def mod(a, n):
    return lax.rem(a + n, n)


def kernel(
    x_hbm, pre_hbm, post_hbm, gs_hbm, us_hbm, br_hbm, oc_hbm, gw_hbm, uw_hbm, dw_hbm,
    ig_hbm, d_out, g_out, u_out,
    *scratch,
):
    s = dict(zip(SCRATCH, scratch))
    W, R, G, GU, silu, dgate, hid = (s[k] for k in ("W", "R", "G", "GU", "si", "dg", "hid"))
    cot, cotT, NG, NS, NX1, NXc = (s[k] for k in ("cot", "cotT", "NG", "NS", "NX1", "NXc"))
    NB, NC = s["NB"], s["NC"]
    RY1, RYo, S, M4, MR, T, XF, K4, KR, KS, U1, UR, TQ, XQ = (
        [s[k, m] for m in range(3)] for k in BUFS
    )
    x_ref, pre_ref, post_ref, br_ref, oc_ref, ig_ref = (
        s[k] for k in ("x", "pre", "post", "br", "oc", "ig")
    )
    ssem, rsem, lsem = s["ssem"], s["rsem"], s["lsem"]
    out = (d_out, g_out, u_out)
    rep, fs, tp = lax.axis_index("rep"), lax.axis_index("fs"), lax.axis_index("tp")
    zl, y = fs // 4, fs % 4
    z = rep * 4 + zl
    x, core = tp // 2, tp % 2
    sib = 1 - core
    half = y // 2
    mate, cross = y + 1 - 2 * (y % 2), 3 - y
    diag = 3 - mate
    zm, zp, z2 = mod(zl - 1, 4), mod(zl + 1, 4), mod(zl + 2, 4)
    xm, xp, x2 = mod(x - 1, 4), mod(x + 1, 4), mod(x + 2, 4)

    def zdev(d):
        zz = mod(z + d, 8)
        return {"rep": zz // 4, "fs": (zz % 4) * 4 + y}

    dev = {
        "m": {"fs": zl * 4 + mate},
        "c": {"fs": zl * 4 + cross},
        "z+": zdev(1),
        "z-": zdev(-1),
        "zz+": zdev(2),
        "zz-": zdev(-2),
        "x+": {"tp": xp * 2 + core},
        "x-": {"tp": xm * 2 + core},
        "s": {"tp": x * 2 + sib},
    }
    ZS = ("z+", "z-")
    XS = ("x+", "x-")

    barrier = pltpu.get_barrier_semaphore()
    for name in dev:
        pl.semaphore_signal(barrier, inc=1, device_id=dev[name], device_id_type=MESH)

    ids = {}
    sends = []
    count = [0]

    def number(key):
        return ids.setdefault(key, len(ids))

    def send(key, src, dst, to):
        if len(sends) == N_SEND:
            sends.pop(0).wait_send()
        c = pltpu.make_async_remote_copy(
            src_ref=src, dst_ref=dst, send_sem=ssem.at[count[0] % N_SEND],
            recv_sem=rsem.at[number(key)], device_id=dev[to], device_id_type=MESH,
        )
        c.start()
        count[0] += 1
        sends.append(c)

    def recv(key, ref):
        pltpu.make_async_copy(ref, ref, rsem.at[number(key)]).wait()

    own = (dw_hbm, gw_hbm, uw_hbm)
    local = {}

    def load(key, src, dst):
        c = pltpu.make_async_copy(src, dst, lsem.at[len(local)])
        c.start()
        local[key] = c

    mine = pl.ds(pl.multiple_of(half * HU, 32), HU)
    other = pl.ds(pl.multiple_of((1 - half) * HU, 32), HU)
    load("br", br_hbm, br_ref)
    load("oc", oc_hbm, oc_ref)
    load("post", post_hbm, post_ref)
    load("x", x_hbm, x_ref)
    load("pre", pre_hbm, pre_ref)
    load("gs", gs_hbm.at[mine], GU.at[0, 0])
    load("us", us_hbm.at[mine], GU.at[0, 1])
    for m in range(3):
        load(("w", m), own[m].at[mine], W.at[m, zl, y])

    def rows_b():
        for key in ("br", "oc", "post"):
            local[key].wait()
        br = br_ref[...].astype(f32)
        inv_b = lax.rsqrt(jnp.mean(br * br, axis=-1, keepdims=True) + eps)
        upst = 0.5 * oc_ref[...].astype(f32) * post_ref[...]
        mean = jnp.mean(upst * br, axis=-1, keepdims=True)
        R[1, 0, tp] = (inv_b * upst - br * (inv_b * inv_b * inv_b) * mean).astype(bf16)

    def rows_n():
        for key in ("x", "pre"):
            local[key].wait()
        xf = x_ref[...].astype(f32)
        inv_x = lax.rsqrt(jnp.mean(xf * xf, axis=-1, keepdims=True) + eps)
        R[0, 0, tp] = (xf * inv_x * pre_ref[...]).astype(bf16)

    ev = [rows_b, rows_n]

    def event(fn, *args):
        ev.append(lambda: fn(*args))

    def enter():
        pl.semaphore_wait(barrier, len(dev))

    event(enter)

    def ag_own(m):
        w = own[m].at[mine]
        send(("o", m), w, W.at[m, zl, y], "m")
        send(("c", m), own[m].at[other], W.at[m, zl, y], "c")
        for to in ZS:
            send(("z", m, 0), w, W.at[m, zl, y], to)

    def ag_y(m, k):
        yy = (mate, cross, diag)[k]
        w = W.at[m, zl, yy]
        recv((("o", m), ("c", m), ("d", m))[k], w)
        if k == 1:
            send(("d", m), w, w, "m")
        for to in ZS:
            send(("z", m, k + 1), w, w, to)

    Q = (pl.ds(0, QU), pl.ds(QU, QU))

    def ag_z(m, k):
        yy = (y, mate, cross, diag)[k]
        recv(("z", m, k), W.at[m, 0, pl.ds(0, 2)])
        for d in range(2):
            w = W.at[m, (zm, zp)[d], yy, Q[d]]
            send(("w", m), w, w, ZS[d])

    def ag_end(m):
        local[("w", m)].wait()
        recv(("w", m), W.at[m, z2])

    for m in range(3):
        event(ag_own, m)
        for k in range(3):
            event(ag_y, m, k)
        for k in range(4):
            event(ag_z, m, k)
        event(ag_end, m)

    C = (pl.ds(0, 1024), pl.ds(1024, 1024))

    def rows_own(n):
        r = R.at[n, 0, tp]
        send(("rc", n), r, R.at[n, 1, tp], "c")
        rows_out(n, 0)

    def rows_cross(n):
        recv(("rc", n), R.at[n, 1, tp])
        rows_out(n, 1)

    def rows_out(n, b):
        r = R.at[n, b, tp]
        for to in XS:
            send(("r", n, b), r, r, to)
        send(("j", n, b), r, r, "s")

    def rows_near(n, b):
        recv(("r", n, b), R.at[n, b, pl.ds(0, 2)])
        for d in range(2):
            slot = (xm, xp)[d] * 2 + core
            r = R.at[n, b, slot, :, C[d]]
            send(("rf", n, b), r, r, XS[d])
        for d in range(2):
            r = R.at[n, b, (xm, xp)[d] * 2 + core]
            send(("j", n, b), r, r, "s")

    def rows_far(n, b):
        r = R.at[n, b, x2 * 2 + core]
        recv(("rf", n, b), r)
        send(("j", n, b), r, r, "s")

    def rows_end(n, b):
        recv(("j", n, b), R.at[n, b, pl.ds(0, 4)])

    for n in range(2):
        event(rows_own, n)
        event(rows_cross, n)
        for b in range(2):
            event(rows_near, n, b)
            event(rows_far, n, b)
            event(rows_end, n, b)

    def gates_out():
        send("gu", gs_hbm.at[other], GU.at[1, 0], "c")
        send("gu", us_hbm.at[other], GU.at[1, 1], "c")

    def factors(b):
        if b == 0:
            local["gs"].wait()
            local["us"].wait()
        else:
            recv("gu", GU.at[1])
        cols = pl.ds(b * 512, 512)

        def body(i, _):
            r = pl.ds(pl.multiple_of(i * 32, 32), 32)
            g, u = GU[b, 0, r, :].astype(f32), GU[b, 1, r, :].astype(f32)
            sg = jax.nn.sigmoid(g)
            v = g * sg
            silu[r, cols] = v
            hid[r, cols] = (v * u).astype(bf16)
            dgate[r, cols] = u * sg * (1.0 + g * (1.0 - sg))
            return 0

        lax.fori_loop(0, HU // 32, body, 0)

    def partial(m, left, off, n):
        def body(c, _):
            cols = pl.ds(pl.multiple_of(c * 512, 512), 512)
            right = R[n, :, :, :, cols].reshape(1024, 512)
            g = jnp.dot(left[off : off + HU, :], right, preferred_element_type=f32).astype(bf16)
            for k in range(4):
                G[m, c, k] = g[:, k * 128 : (k + 1) * 128]
            return 0

        lax.fori_loop(0, 4, body, 0)

    def hidden_grad():
        def body(t, _):
            right = R[1, t // 2, pl.ds((t % 2) * 4, 4)].reshape(256, 2048)
            left = jnp.concatenate([W[0, k // 4, k % 4] for k in range(16)], axis=1)
            hg = lax.dot_general(
                left, right, (((1,), (1,)), ((), ())), preferred_element_type=f32
            )
            cols = pl.ds(pl.multiple_of(t * 256, 256), 256)
            cot[pl.ds(0, HU), cols] = (hg * dgate[:, cols]).astype(bf16)
            cot[pl.ds(HU, HU), cols] = (hg * silu[:, cols]).astype(bf16)
            return 0

        lax.fori_loop(0, 4, body, 0)

    def turn():
        for k in range(8):
            cotT[k * 128 : (k + 1) * 128, :] = cot[:, k * 128 : (k + 1) * 128].T

    def normed_grad(h):
        def body(c, _):
            right = jnp.concatenate(
                [jnp.concatenate([W[1, c, k], W[2, c, k]], axis=0) for k in range(4)], axis=1
            )
            g = jnp.dot(cotT[...], right, preferred_element_type=f32).astype(bf16)
            cols = pl.ds(pl.multiple_of(c * 512, 512), 512)
            NG[:, :, :, :, cols] = g.reshape(2, 4, 2, 64, 512)
            return 0

        lax.fori_loop(2 * h, 2 * h + 2, body, 0)
        send(("np", h), NG.at[:, :, sib, :, C[h]], NS.at[:, :, :, C[h]], "s")

    event(gates_out)
    event(factors, 0)
    event(factors, 1)
    event(partial, 0, hid, 0, 1)
    event(hidden_grad)
    event(partial, 1, cot, 0, 0)
    event(partial, 2, cot, HU, 0)
    event(turn)
    event(normed_grad, 0)
    event(normed_grad, 1)

    def ng_first(h):
        recv(("np", h), NS.at[:, :, :, C[h]])
        for b in range(2):
            for k in range(4):
                NG[b, k, core, :, C[h]] = NG[b, k, core, :, C[h]] + NS[b, k, :, C[h]]
        send(("n1", h), NG.at[:, x2, core, :, C[h]], NX1.at[h], XS[h])
        send("n", NG.at[:, (xm, xp)[h], core, :, C[h]], NXc.at[2 + h], XS[1 - h])

    def ng_second(h):
        nxt = (xp, xm)[h]
        recv(("n1", h), NX1.at[h])
        for b in range(2):
            NG[b, nxt, core, :, C[h]] = NG[b, nxt, core, :, C[h]] + NX1[h, b]
        send("n", NG.at[:, nxt, core, :, C[h]], NXc.at[h], XS[h])

    def ng_sum(b):
        return jnp.concatenate(
            [
                NG[b, x, core, :, C[h]].astype(f32)
                + NXc[h, b].astype(f32)
                + NXc[2 + h, b].astype(f32)
                for h in range(2)
            ],
            axis=1,
        )

    def ng_third():
        recv("n", NXc)
        NB[...] = ng_sum(1).astype(bf16)
        send("nc", NB, NC, "c")

    def ng_end():
        recv("nc", NC)
        w = (ng_sum(0) + NC[...].astype(f32)) * pre_ref[...]
        xv = x_ref[...].astype(f32)
        inv = lax.rsqrt(jnp.mean(xv * xv, axis=-1, keepdims=True) + eps)
        ig_ref[...] = (
            oc_ref[...].astype(f32)
            + inv * w
            - xv * (inv * inv * inv) * jnp.mean(w * xv, axis=-1, keepdims=True)
        ).astype(bf16)
        load("ig", ig_ref, ig_hbm)

    for h in range(2):
        event(ng_first, h)
        event(ng_second, h)
    event(ng_third)
    event(ng_end)

    CH = (zl, zm, zp, z2)
    OWN = {k: (mod(zl + k, 4), mod(z + k, 8) // 4) for k in (4, 3, 2, 1, -1, -2, -3)}

    def add3(a, b, c):
        return (a.astype(f32) + b.astype(f32) + c.astype(f32)).astype(bf16)

    def from_rep(d):
        return mod(z + (-2, 2)[d], 8) // 4

    def rs_first(m):
        p = pl.ds(0, HU - NQ[m])
        for c in range(4):
            send(("a", m, c), G.at[m, CH[c], diag, p], RY1[m].at[c], "m")
        for c in range(4):
            send(("C", m, c), G.at[m, CH[c], mate, p], RYo[m].at[c], "m")

    def rs_second(m, c):
        p = pl.ds(0, HU - NQ[m])
        recv(("a", m, c), RY1[m].at[c])
        G[m, CH[c], cross, p] = G[m, CH[c], cross, p] + RY1[m][c]
        send(("C", m, c), G.at[m, CH[c], cross, p], S[m].at[CH[c], half], "c")

    def rs_third(m, c):
        p = pl.ds(0, HU - NQ[m])
        recv(("C", m, c), S[m].at[CH[c]])
        S[m][CH[c], half] = G[m, CH[c], y, p] + RYo[m][c]
        if c == 0:
            slot, h = OWN[4]
            for d in range(2):
                send(("M", m, 4), S[m].at[slot, h, part(m, d)], M4[m].at[d], ZS[d])

    def part(m, d):
        n = (HU - NQ[m]) // 2
        return pl.ds(d * n, n)

    def rs_ring(m, k):
        recv(("M", m, k + 1), M4[m] if k == 3 else MR[m].at[2 - k])
        for d in range(2):
            slot, h = OWN[(k, -k)[d]]
            if k == 3:
                r = part(m, d)
                S[m][slot, h, r] = S[m][slot, h, r] + M4[m][d]
            else:
                S[m][slot, h] = S[m][slot, h] + MR[m][2 - k, d]
            send(("M", m, k), S[m].at[slot, h], MR[m].at[3 - k, d], ZS[d])

    def rows_at(start, n):
        return pl.ds(pl.multiple_of(start, 16), n)

    def rs_own(m):
        recv(("M", m, 1), MR[m].at[2])
        T[m][...] = add3(S[m][zl, rep], MR[m][2, 0], MR[m][2, 1])
        for d in range(2):
            r = part(m, d)
            send(("x", m), T[m].at[r], XF[m].at[r], ("zz+", "zz-")[d])
        load(("out", m), T[m], out[m].at[rows_at(rep * HU, HU - NQ[m])])

    def rs_swap(m):
        recv(("x", m), XF[m])
        n = (HU - NQ[m]) // 2
        for d in range(2):
            dst = out[m].at[rows_at(from_rep(d) * HU + d * n, n)]
            send(("e", m), XF[m].at[part(m, d)], dst, ("zz+", "zz-")[d])

    def rows_q(m, h, d, parts):
        n = NQ[m]
        return rows_at(HU - n + h * (n // 2) + d * (n // 4), n // parts)

    def qs_first(m):
        slot, h = OWN[4]
        for d in range(2):
            send(("K", m, 4), G.at[m, slot, :, rows_q(m, h, d, 4)], K4[m].at[d], ZS[d])

    def qs_ring(m, k):
        recv(("K", m, k + 1), K4[m] if k == 3 else KR[m].at[2 - k])
        for d in range(2):
            slot, h = OWN[(k, -k)[d]]
            if k == 3:
                r = rows_q(m, h, d, 4)
                G[m, slot, :, r] = G[m, slot, :, r] + K4[m][d]
            else:
                r = rows_q(m, h, 0, 2)
                G[m, slot, :, r] = G[m, slot, :, r] + KR[m][2 - k, d]
            src = G.at[m, slot, :, rows_q(m, h, 0, 2)]
            send(("K", m, k), src, KR[m].at[3 - k, d], ZS[d])

    def qs_own(m):
        recv(("K", m, 1), KR[m].at[2])
        KS[m][...] = add3(G[m, zl, :, rows_q(m, rep, 0, 2)], KR[m][2, 0], KR[m][2, 1])
        send(("u", m), KS[m].at[diag], U1[m], "m")
        send(("U", m), KS[m].at[mate], UR[m].at[0], "m")

    def qs_cross(m):
        recv(("u", m), U1[m])
        KS[m][cross] = KS[m][cross] + U1[m][...]
        send(("U", m), KS[m].at[cross], UR[m].at[1], "c")

    def qs_sum(m):
        recv(("U", m), UR[m])
        TQ[m][half] = KS[m][y] + UR[m][0]
        TQ[m][1 - half] = UR[m][1]
        n = NQ[m] // 2
        for d in range(2):
            send(("v", m), TQ[m].at[d], XQ[m].at[d], ("zz+", "zz-")[d])
            load(("out", m, d), TQ[m].at[d], out[m].at[rows_at((d + 1) * HU - 2 * n + rep * n, n)])

    def qs_swap(m):
        recv(("v", m), XQ[m])
        n = NQ[m] // 2
        for d in range(2):
            dst = out[m].at[rows_at((d + 1) * HU - 2 * n + from_rep(d) * n, n)]
            send(("e", m), XQ[m].at[d], dst, ("zz+", "zz-")[d])

    def rs_end(m):
        recv(("e", m), G.at[m, 0, 0])

    for m in range(3):
        event(rs_first, m)
        for c in range(4):
            event(rs_second, m, c)
            event(rs_third, m, c)
        for k in (3, 2, 1):
            event(rs_ring, m, k)
        event(rs_own, m)
        event(rs_swap, m)
        event(qs_first, m)
        for k in (3, 2, 1):
            event(qs_ring, m, k)
        event(qs_own, m)
        event(qs_cross, m)
        event(qs_sum, m)
        event(qs_swap, m)
        event(rs_end, m)

    for k in ORDER:
        ev[k]()
    assert sorted(ORDER) == list(range(len(ev))) and len(ids) <= N_RECV
    for c in sends:
        c.wait_send()
    for key in local:
        if key == "ig" or key[0] == "out":
            local[key].wait()


V, SEM = pltpu.VMEM, pltpu.SemaphoreType.DMA
SCRATCH = {
    "W": V((3, 4, 4, HU, 128), bf16),
    "R": V((2, 2, 8, 64, 2048), bf16),
    "G": V((3, 4, 4, HU, 128), bf16),
    "GU": V((2, 2, HU, 512), bf16),
    "si": V((HU, 1024), f32),
    "dg": V((HU, 1024), f32),
    "hid": V((HU, 1024), bf16),
    "cot": V((2 * HU, 1024), bf16),
    "cotT": V((1024, 2 * HU), bf16),
    "NG": V((2, 4, 2, 64, 2048), bf16),
    "NS": V((2, 4, 64, 2048), bf16),
    "NX1": V((2, 2, 64, 1024), bf16),
    "NXc": V((4, 2, 64, 1024), bf16),
    "NB": V((64, 2048), bf16),
    "NC": V((64, 2048), bf16),
    "x": V((64, 2048), bf16),
    "br": V((64, 2048), bf16),
    "oc": V((64, 2048), bf16),
    "ig": V((64, 2048), bf16),
    "pre": V((1, 2048), f32),
    "post": V((1, 2048), f32),
    "ssem": SEM((N_SEND,)),
    "rsem": SEM((N_RECV,)),
    "lsem": SEM((N_LOCAL,)),
}


BUFS = ("RY1", "RYo", "S", "M4", "MR", "T", "XF", "K4", "KR", "KS", "U1", "UR", "TQ", "XQ")
for m in range(3):
    p, h = HU - NQ[m], NQ[m] // 2
    shapes = (
        (4, p), (4, p), (4, 2, p), (2, p // 2), (3, 2, p), (p,), (p,),
        (2, 4, h // 2), (3, 2, 4, h), (4, h), (h,), (2, h), (2, h), (2, h),
    )
    for k, shape in zip(BUFS, shapes):
        SCRATCH[k, m] = V((*shape, 128), bf16)


def finish(*refs):
    ins, outs, (row, half, full, sem) = refs[:4], refs[4:8], refs[8:]
    bufs = [row] + [half.at[m] for m in range(3)]
    res = [row] + [full.at[m] for m in range(3)]
    loads = [pltpu.make_async_copy(ins[k], bufs[k], sem.at[k]) for k in range(4)]
    stores = [pltpu.make_async_copy(res[k], outs[k], sem.at[4 + k]) for k in range(4)]
    for c in loads:
        c.start()
    for k in range(4):
        loads[k].wait()
        if k:
            full[k - 1] = half[k - 1].astype(f32)
        stores[k].start()
    for c in stores:
        c.wait()


def per_device(x, pre, post, gs, us, br, oc, gw, uw, dw):
    hbm = pl.BlockSpec(memory_space=pl.ANY)
    sds = jax.ShapeDtypeStruct
    parts = pl.pallas_call(
        kernel,
        out_shape=(sds((64, 2048), bf16), *[sds((2 * HU, 128), bf16)] * 3),
        in_specs=[hbm] * 10,
        out_specs=(hbm,) * 4,
        scratch_shapes=list(SCRATCH.values()),
        compiler_params=pltpu.CompilerParams(
            collective_id=0, has_side_effects=True, vmem_limit_bytes=67_000_000
        ),
        name="ffn_backward",
    )(x, pre.reshape(1, -1), post.reshape(1, -1), gs.T, us.T, br, oc, gw.T, uw.T, dw.T)
    ig, dg, gg, ug = pl.pallas_call(
        finish,
        out_shape=(sds((64, 2048), bf16), *[sds((2 * HU, 128), f32)] * 3),
        in_specs=[hbm] * 4,
        out_specs=(hbm,) * 4,
        scratch_shapes=[
            V((64, 2048), bf16), V((3, 2 * HU, 128), bf16), V((3, 2 * HU, 128), f32), SEM((8,)),
        ],
        name="finish",
    )(*parts)
    return ig, gg.T, ug.T, dg.T


def solution(mesh):
    return jax.shard_map(
        per_device,
        mesh=mesh,
        in_specs=(
            P(("rep", "fs", "tp"), None),
            P(),
            P(),
            P(("rep", "fs"), "tp"),
            P(("rep", "fs"), "tp"),
            P(("rep", "fs", "tp"), None),
            P(("rep", "fs", "tp"), None),
            P("fs", "tp"),
            P("fs", "tp"),
            P("fs", "tp"),
        ),
        out_specs=(P(("rep", "fs", "tp"), None), P("fs", "tp"), P("fs", "tp"), P("fs", "tp")),
        check_vma=False,
    )
```

```python
import jax
import jax.numpy as jnp
from jax import lax
from jax.experimental import pallas as pl
from jax.experimental.pallas import tpu as pltpu
from jax.sharding import PartitionSpec as P

MESH = pl.DeviceIdType.MESH
bf16, f32 = jnp.bfloat16, jnp.float32
eps = 1e-06

HU = 352
QU = HU // 2
NQ = (192, 192, 192)
N_RECV, N_SEND, N_LOCAL = 108, 48, 20
ORDER = (
    2, 3, 21, 0, 38, 47, 12, 1, 30, 4, 5, 22, 23, 25, 16, 40, 8, 6, 39, 24, 9, 14, 32, 26, 46, 27,
    41, 7, 13, 15, 42, 31, 10, 43, 28, 33, 18, 34, 17, 35, 19, 11, 44, 29, 48, 45, 49, 36, 50, 85,
    51, 52, 37, 54, 108, 58, 131, 59, 60, 86, 61, 72, 53, 74, 117, 20, 55, 56, 109, 57, 94, 132, 95,
    76, 71, 118, 120, 87, 122, 62, 64, 110, 124, 78, 119, 133, 123, 67, 125, 63, 88, 101, 97, 99,
    96, 134, 65, 102, 98, 73, 121, 126, 89, 100, 103, 68, 77, 111, 75, 79, 135, 90, 80, 127, 104,
    136, 91, 66, 112, 81, 137, 128, 105, 113, 92, 82, 114, 138, 129, 69, 106, 83, 115, 130, 107, 84,
    70, 139, 116, 93,
)


def mod(a, n):
    return lax.rem(a + n, n)


def kernel(
    x_hbm, pre_hbm, post_hbm, gs_hbm, us_hbm, br_hbm, oc_hbm, gw_hbm, uw_hbm, dw_hbm,
    ig_hbm, d_out, g_out, u_out,
    *scratch,
):
    s = dict(zip(SCRATCH, scratch))
    W, R, G, GU, silu, dgate, hid = (s[k] for k in ("W", "R", "G", "GU", "si", "dg", "hid"))
    cot, cotT, NG, NS, NX1, NXc = (s[k] for k in ("cot", "cotT", "NG", "NS", "NX1", "NXc"))
    NB, NC = s["NB"], s["NC"]
    RY1, RYo, S, M4, MR, T, XF, K4, KR, KS, U1, UR, TQ, XQ = (
        [s[k, m] for m in range(3)] for k in BUFS
    )
    x_ref, pre_ref, post_ref, br_ref, oc_ref, ig_ref = (
        s[k] for k in ("x", "pre", "post", "br", "oc", "ig")
    )
    ssem, rsem, lsem = s["ssem"], s["rsem"], s["lsem"]
    out = (d_out, g_out, u_out)
    rep, fs, tp = lax.axis_index("rep"), lax.axis_index("fs"), lax.axis_index("tp")
    zl, y = fs // 4, fs % 4
    z = rep * 4 + zl
    x, core = tp // 2, tp % 2
    sib = 1 - core
    half = y // 2
    mate, cross = y + 1 - 2 * (y % 2), 3 - y
    diag = 3 - mate
    zm, zp, z2 = mod(zl - 1, 4), mod(zl + 1, 4), mod(zl + 2, 4)
    xm, xp, x2 = mod(x - 1, 4), mod(x + 1, 4), mod(x + 2, 4)

    def zdev(d):
        zz = mod(z + d, 8)
        return {"rep": zz // 4, "fs": (zz % 4) * 4 + y}

    dev = {
        "m": {"fs": zl * 4 + mate},
        "c": {"fs": zl * 4 + cross},
        "z+": zdev(1),
        "z-": zdev(-1),
        "zz+": zdev(2),
        "zz-": zdev(-2),
        "x+": {"tp": xp * 2 + core},
        "x-": {"tp": xm * 2 + core},
        "s": {"tp": x * 2 + sib},
    }
    ZS = ("z+", "z-")
    XS = ("x+", "x-")

    barrier = pltpu.get_barrier_semaphore()
    for name in dev:
        pl.semaphore_signal(barrier, inc=1, device_id=dev[name], device_id_type=MESH)

    ids = {}
    sends = []
    count = [0]

    def number(key):
        return ids.setdefault(key, len(ids))

    def send(key, src, dst, to):
        if len(sends) == N_SEND:
            sends.pop(0).wait_send()
        c = pltpu.make_async_remote_copy(
            src_ref=src, dst_ref=dst, send_sem=ssem.at[count[0] % N_SEND],
            recv_sem=rsem.at[number(key)], device_id=dev[to], device_id_type=MESH,
        )
        c.start()
        count[0] += 1
        sends.append(c)

    def recv(key, ref):
        pltpu.make_async_copy(ref, ref, rsem.at[number(key)]).wait()

    own = (dw_hbm, gw_hbm, uw_hbm)
    local = {}

    def load(key, src, dst):
        c = pltpu.make_async_copy(src, dst, lsem.at[len(local)])
        c.start()
        local[key] = c

    mine = pl.ds(pl.multiple_of(half * HU, 32), HU)
    other = pl.ds(pl.multiple_of((1 - half) * HU, 32), HU)
    load("br", br_hbm, br_ref)
    load("oc", oc_hbm, oc_ref)
    load("post", post_hbm, post_ref)
    load("x", x_hbm, x_ref)
    load("pre", pre_hbm, pre_ref)
    load("gs", gs_hbm.at[mine], GU.at[0, 0])
    load("us", us_hbm.at[mine], GU.at[0, 1])
    for m in range(3):
        load(("w", m), own[m].at[mine], W.at[m, zl, y])

    def rows_b():
        for key in ("br", "oc", "post"):
            local[key].wait()
        br = br_ref[...].astype(f32)
        inv_b = lax.rsqrt(jnp.mean(br * br, axis=-1, keepdims=True) + eps)
        upst = 0.5 * oc_ref[...].astype(f32) * post_ref[...]
        mean = jnp.mean(upst * br, axis=-1, keepdims=True)
        R[1, 0, tp] = (inv_b * upst - br * (inv_b * inv_b * inv_b) * mean).astype(bf16)

    def rows_n():
        for key in ("x", "pre"):
            local[key].wait()
        xf = x_ref[...].astype(f32)
        inv_x = lax.rsqrt(jnp.mean(xf * xf, axis=-1, keepdims=True) + eps)
        R[0, 0, tp] = (xf * inv_x * pre_ref[...]).astype(bf16)

    ev = [rows_b, rows_n]

    def event(fn, *args):
        ev.append(lambda: fn(*args))

    def enter():
        pl.semaphore_wait(barrier, len(dev))

    event(enter)

    def ag_own(m):
        w = own[m].at[mine]
        send(("o", m), w, W.at[m, zl, y], "m")
        send(("c", m), own[m].at[other], W.at[m, zl, y], "c")
        for to in ZS:
            send(("z", m, 0), w, W.at[m, zl, y], to)

    def ag_y(m, k):
        yy = (mate, cross, diag)[k]
        w = W.at[m, zl, yy]
        recv((("o", m), ("c", m), ("d", m))[k], w)
        if k == 1:
            send(("d", m), w, w, "m")
        for to in ZS:
            send(("z", m, k + 1), w, w, to)

    Q = (pl.ds(0, QU), pl.ds(QU, QU))

    def ag_z(m, k):
        yy = (y, mate, cross, diag)[k]
        recv(("z", m, k), W.at[m, 0, pl.ds(0, 2)])
        for d in range(2):
            w = W.at[m, (zm, zp)[d], yy, Q[d]]
            send(("w", m), w, w, ZS[d])

    def ag_end(m):
        local[("w", m)].wait()
        recv(("w", m), W.at[m, z2])

    for m in range(3):
        event(ag_own, m)
        for k in range(3):
            event(ag_y, m, k)
        for k in range(4):
            event(ag_z, m, k)
        event(ag_end, m)

    C = (pl.ds(0, 1024), pl.ds(1024, 1024))

    def rows_own(n):
        r = R.at[n, 0, tp]
        send(("rc", n), r, R.at[n, 1, tp], "c")
        rows_out(n, 0)

    def rows_cross(n):
        recv(("rc", n), R.at[n, 1, tp])
        rows_out(n, 1)

    def rows_out(n, b):
        r = R.at[n, b, tp]
        for to in XS:
            send(("r", n, b), r, r, to)
        send(("j", n, b), r, r, "s")

    def rows_near(n, b):
        recv(("r", n, b), R.at[n, b, pl.ds(0, 2)])
        for d in range(2):
            slot = (xm, xp)[d] * 2 + core
            r = R.at[n, b, slot, :, C[d]]
            send(("rf", n, b), r, r, XS[d])
        for d in range(2):
            r = R.at[n, b, (xm, xp)[d] * 2 + core]
            send(("j", n, b), r, r, "s")

    def rows_far(n, b):
        r = R.at[n, b, x2 * 2 + core]
        recv(("rf", n, b), r)
        send(("j", n, b), r, r, "s")

    def rows_end(n, b):
        recv(("j", n, b), R.at[n, b, pl.ds(0, 4)])

    for n in range(2):
        event(rows_own, n)
        event(rows_cross, n)
        for b in range(2):
            event(rows_near, n, b)
            event(rows_far, n, b)
            event(rows_end, n, b)

    def gates_out():
        send("gu", gs_hbm.at[other], GU.at[1, 0], "c")
        send("gu", us_hbm.at[other], GU.at[1, 1], "c")

    def factors(b):
        if b == 0:
            local["gs"].wait()
            local["us"].wait()
        else:
            recv("gu", GU.at[1])
        cols = pl.ds(b * 512, 512)

        def body(i, _):
            r = pl.ds(pl.multiple_of(i * 32, 32), 32)
            g, u = GU[b, 0, r, :].astype(f32), GU[b, 1, r, :].astype(f32)
            sg = jax.nn.sigmoid(g)
            v = g * sg
            silu[r, cols] = v
            hid[r, cols] = (v * u).astype(bf16)
            dgate[r, cols] = u * sg * (1.0 + g * (1.0 - sg))
            return 0

        lax.fori_loop(0, HU // 32, body, 0)

    CH = (zl, zm, zp, z2)

    def partial(m, c):
        n, left = ((1, hid), (0, cot.at[:HU]), (0, cot.at[HU:]))[m]
        cols = pl.ds(pl.multiple_of(CH[c] * 512, 512), 512)
        right = R[n, :, :, :, cols].reshape(1024, 512)
        g = jnp.dot(left[...], right, preferred_element_type=f32).astype(bf16)
        for k in range(4):
            G[m, CH[c], k] = g[:, k * 128 : (k + 1) * 128]
        send(("a", m, c), G.at[m, CH[c], diag, pl.ds(0, HU - NQ[m])], RY1[m].at[c], "m")

    def hidden_grad():
        def body(t, _):
            right = R[1, t].reshape(512, 2048)
            left = jnp.concatenate([W[0, k // 4, k % 4] for k in range(16)], axis=1)
            hg = lax.dot_general(
                left, right, (((1,), (1,)), ((), ())), preferred_element_type=f32
            )
            cols = pl.ds(pl.multiple_of(t * 512, 512), 512)
            cot[pl.ds(0, HU), cols] = (hg * dgate[:, cols]).astype(bf16)
            cot[pl.ds(HU, HU), cols] = (hg * silu[:, cols]).astype(bf16)
            return 0

        lax.fori_loop(0, 2, body, 0)

    def turn():
        for k in range(8):
            cotT[k * 128 : (k + 1) * 128, :] = cot[:, k * 128 : (k + 1) * 128].T

    def normed_grad(h):
        def body(c, _):
            right = jnp.concatenate(
                [jnp.concatenate([W[1, c, k], W[2, c, k]], axis=0) for k in range(4)], axis=1
            )
            g = jnp.dot(cotT[...], right, preferred_element_type=f32).astype(bf16)
            cols = pl.ds(pl.multiple_of(c * 512, 512), 512)
            NG[:, :, :, :, cols] = g.reshape(2, 4, 2, 64, 512)
            return 0

        lax.fori_loop(2 * h, 2 * h + 2, body, 0)
        send(("np", h), NG.at[:, :, sib, :, C[h]], NS.at[:, :, :, C[h]], "s")

    event(gates_out)
    event(factors, 0)
    event(factors, 1)
    event(hidden_grad)
    for m in range(3):
        for c in range(4):
            event(partial, m, c)
    event(turn)
    event(normed_grad, 0)
    event(normed_grad, 1)

    def ng_first(h):
        recv(("np", h), NS.at[:, :, :, C[h]])
        for b in range(2):
            for k in range(4):
                NG[b, k, core, :, C[h]] = NG[b, k, core, :, C[h]] + NS[b, k, :, C[h]]
        send(("n1", h), NG.at[:, x2, core, :, C[h]], NX1.at[h], XS[h])
        send("n", NG.at[:, (xm, xp)[h], core, :, C[h]], NXc.at[2 + h], XS[1 - h])

    def ng_second(h):
        nxt = (xp, xm)[h]
        recv(("n1", h), NX1.at[h])
        for b in range(2):
            NG[b, nxt, core, :, C[h]] = NG[b, nxt, core, :, C[h]] + NX1[h, b]
        send("n", NG.at[:, nxt, core, :, C[h]], NXc.at[h], XS[h])

    def ng_sum(b):
        return jnp.concatenate(
            [
                NG[b, x, core, :, C[h]].astype(f32)
                + NXc[h, b].astype(f32)
                + NXc[2 + h, b].astype(f32)
                for h in range(2)
            ],
            axis=1,
        )

    def ng_third():
        recv("n", NXc)
        NB[...] = ng_sum(1).astype(bf16)
        send("nc", NB, NC, "c")

    def ng_end():
        recv("nc", NC)
        w = (ng_sum(0) + NC[...].astype(f32)) * pre_ref[...]
        xv = x_ref[...].astype(f32)
        inv = lax.rsqrt(jnp.mean(xv * xv, axis=-1, keepdims=True) + eps)
        ig_ref[...] = (
            oc_ref[...].astype(f32)
            + inv * w
            - xv * (inv * inv * inv) * jnp.mean(w * xv, axis=-1, keepdims=True)
        ).astype(bf16)
        load("ig", ig_ref, ig_hbm)

    for h in range(2):
        event(ng_first, h)
        event(ng_second, h)
    event(ng_third)
    event(ng_end)

    OWN = {k: (mod(zl + k, 4), mod(z + k, 8) // 4) for k in (4, 3, 2, 1, -1, -2, -3)}

    def add3(a, b, c):
        return (a.astype(f32) + b.astype(f32) + c.astype(f32)).astype(bf16)

    def from_rep(d):
        return mod(z + (-2, 2)[d], 8) // 4

    def rs_first(m):
        p = pl.ds(0, HU - NQ[m])
        for c in range(4):
            send(("C", m, c), G.at[m, CH[c], mate, p], RYo[m].at[c], "m")

    def rs_second(m, c):
        p = pl.ds(0, HU - NQ[m])
        recv(("a", m, c), RY1[m].at[c])
        G[m, CH[c], cross, p] = G[m, CH[c], cross, p] + RY1[m][c]
        send(("C", m, c), G.at[m, CH[c], cross, p], S[m].at[CH[c], half], "c")

    def rs_third(m, c):
        p = pl.ds(0, HU - NQ[m])
        recv(("C", m, c), S[m].at[CH[c]])
        S[m][CH[c], half] = G[m, CH[c], y, p] + RYo[m][c]
        if c == 0:
            slot, h = OWN[4]
            for d in range(2):
                send(("M", m, 4), S[m].at[slot, h, part(m, d)], M4[m].at[d], ZS[d])

    def part(m, d):
        n = (HU - NQ[m]) // 2
        return pl.ds(d * n, n)

    def rs_ring(m, k):
        recv(("M", m, k + 1), M4[m] if k == 3 else MR[m].at[2 - k])
        for d in range(2):
            slot, h = OWN[(k, -k)[d]]
            if k == 3:
                r = part(m, d)
                S[m][slot, h, r] = S[m][slot, h, r] + M4[m][d]
            else:
                S[m][slot, h] = S[m][slot, h] + MR[m][2 - k, d]
            send(("M", m, k), S[m].at[slot, h], MR[m].at[3 - k, d], ZS[d])

    def rows_at(start, n):
        return pl.ds(pl.multiple_of(start, 16), n)

    def rs_own(m):
        recv(("M", m, 1), MR[m].at[2])
        T[m][...] = add3(S[m][zl, rep], MR[m][2, 0], MR[m][2, 1])
        for d in range(2):
            r = part(m, d)
            send(("x", m), T[m].at[r], XF[m].at[r], ("zz+", "zz-")[d])
        load(("out", m), T[m], out[m].at[rows_at(rep * HU, HU - NQ[m])])

    def rs_swap(m):
        recv(("x", m), XF[m])
        n = (HU - NQ[m]) // 2
        for d in range(2):
            dst = out[m].at[rows_at(from_rep(d) * HU + d * n, n)]
            send(("e", m), XF[m].at[part(m, d)], dst, ("zz+", "zz-")[d])

    def rows_q(m, h, d, parts):
        n = NQ[m]
        return rows_at(HU - n + h * (n // 2) + d * (n // 4), n // parts)

    def qs_first(m):
        slot, h = OWN[4]
        for d in range(2):
            send(("K", m, 4), G.at[m, slot, :, rows_q(m, h, d, 4)], K4[m].at[d], ZS[d])

    def qs_ring(m, k):
        recv(("K", m, k + 1), K4[m] if k == 3 else KR[m].at[2 - k])
        for d in range(2):
            slot, h = OWN[(k, -k)[d]]
            if k == 3:
                r = rows_q(m, h, d, 4)
                G[m, slot, :, r] = G[m, slot, :, r] + K4[m][d]
            else:
                r = rows_q(m, h, 0, 2)
                G[m, slot, :, r] = G[m, slot, :, r] + KR[m][2 - k, d]
            src = G.at[m, slot, :, rows_q(m, h, 0, 2)]
            send(("K", m, k), src, KR[m].at[3 - k, d], ZS[d])

    def qs_own(m):
        recv(("K", m, 1), KR[m].at[2])
        KS[m][...] = add3(G[m, zl, :, rows_q(m, rep, 0, 2)], KR[m][2, 0], KR[m][2, 1])
        send(("u", m), KS[m].at[diag], U1[m], "m")
        send(("U", m), KS[m].at[mate], UR[m].at[0], "m")

    def qs_cross(m):
        recv(("u", m), U1[m])
        KS[m][cross] = KS[m][cross] + U1[m][...]
        send(("U", m), KS[m].at[cross], UR[m].at[1], "c")

    def qs_sum(m):
        recv(("U", m), UR[m])
        TQ[m][half] = KS[m][y] + UR[m][0]
        TQ[m][1 - half] = UR[m][1]
        n = NQ[m] // 2
        for d in range(2):
            send(("v", m), TQ[m].at[d], XQ[m].at[d], ("zz+", "zz-")[d])
            load(("out", m, d), TQ[m].at[d], out[m].at[rows_at((d + 1) * HU - 2 * n + rep * n, n)])

    def qs_swap(m):
        recv(("v", m), XQ[m])
        n = NQ[m] // 2
        for d in range(2):
            dst = out[m].at[rows_at((d + 1) * HU - 2 * n + from_rep(d) * n, n)]
            send(("e", m), XQ[m].at[d], dst, ("zz+", "zz-")[d])

    def rs_end(m):
        recv(("e", m), G.at[m, 0, 0])

    for m in range(3):
        event(rs_first, m)
        for c in range(4):
            event(rs_second, m, c)
            event(rs_third, m, c)
        for k in (3, 2, 1):
            event(rs_ring, m, k)
        event(rs_own, m)
        event(rs_swap, m)
        event(qs_first, m)
        for k in (3, 2, 1):
            event(qs_ring, m, k)
        event(qs_own, m)
        event(qs_cross, m)
        event(qs_sum, m)
        event(qs_swap, m)
        event(rs_end, m)

    for k in ORDER:
        ev[k]()
    assert sorted(ORDER) == list(range(len(ev))) and len(ids) <= N_RECV
    for c in sends:
        c.wait_send()
    for key in local:
        if key == "ig" or key[0] == "out":
            local[key].wait()


V, SEM = pltpu.VMEM, pltpu.SemaphoreType.DMA
SCRATCH = {
    "W": V((3, 4, 4, HU, 128), bf16),
    "R": V((2, 2, 8, 64, 2048), bf16),
    "G": V((3, 4, 4, HU, 128), bf16),
    "GU": V((2, 2, HU, 512), bf16),
    "si": V((HU, 1024), f32),
    "dg": V((HU, 1024), f32),
    "hid": V((HU, 1024), bf16),
    "cot": V((2 * HU, 1024), bf16),
    "cotT": V((1024, 2 * HU), bf16),
    "NG": V((2, 4, 2, 64, 2048), bf16),
    "NS": V((2, 4, 64, 2048), bf16),
    "NX1": V((2, 2, 64, 1024), bf16),
    "NXc": V((4, 2, 64, 1024), bf16),
    "NB": V((64, 2048), bf16),
    "NC": V((64, 2048), bf16),
    "x": V((64, 2048), bf16),
    "br": V((64, 2048), bf16),
    "oc": V((64, 2048), bf16),
    "ig": V((64, 2048), bf16),
    "pre": V((1, 2048), f32),
    "post": V((1, 2048), f32),
    "ssem": SEM((N_SEND,)),
    "rsem": SEM((N_RECV,)),
    "lsem": SEM((N_LOCAL,)),
}


BUFS = ("RY1", "RYo", "S", "M4", "MR", "T", "XF", "K4", "KR", "KS", "U1", "UR", "TQ", "XQ")
for m in range(3):
    p, h = HU - NQ[m], NQ[m] // 2
    shapes = (
        (4, p), (4, p), (4, 2, p), (2, p // 2), (3, 2, p), (p,), (p,),
        (2, 4, h // 2), (3, 2, 4, h), (4, h), (h,), (2, h), (2, h), (2, h),
    )
    for k, shape in zip(BUFS, shapes):
        SCRATCH[k, m] = V((*shape, 128), bf16)


def finish(*refs):
    ins, outs, (row, half, full, sem) = refs[:4], refs[4:8], refs[8:]
    bufs = [row] + [half.at[m] for m in range(3)]
    res = [row] + [full.at[m] for m in range(3)]
    loads = [pltpu.make_async_copy(ins[k], bufs[k], sem.at[k]) for k in range(4)]
    stores = [pltpu.make_async_copy(res[k], outs[k], sem.at[4 + k]) for k in range(4)]
    for c in loads:
        c.start()
    for k in range(4):
        loads[k].wait()
        if k:
            full[k - 1] = half[k - 1].astype(f32)
        stores[k].start()
    for c in stores:
        c.wait()


def per_device(x, pre, post, gs, us, br, oc, gw, uw, dw):
    hbm = pl.BlockSpec(memory_space=pl.ANY)
    sds = jax.ShapeDtypeStruct
    parts = pl.pallas_call(
        kernel,
        out_shape=(sds((64, 2048), bf16), *[sds((2 * HU, 128), bf16)] * 3),
        in_specs=[hbm] * 10,
        out_specs=(hbm,) * 4,
        scratch_shapes=list(SCRATCH.values()),
        compiler_params=pltpu.CompilerParams(
            collective_id=0, has_side_effects=True, vmem_limit_bytes=67_000_000
        ),
        name="ffn_backward",
    )(x, pre.reshape(1, -1), post.reshape(1, -1), gs.T, us.T, br, oc, gw.T, uw.T, dw.T)
    ig, dg, gg, ug = pl.pallas_call(
        finish,
        out_shape=(sds((64, 2048), bf16), *[sds((2 * HU, 128), f32)] * 3),
        in_specs=[hbm] * 4,
        out_specs=(hbm,) * 4,
        scratch_shapes=[
            V((64, 2048), bf16), V((3, 2 * HU, 128), bf16), V((3, 2 * HU, 128), f32), SEM((8,)),
        ],
        name="finish",
    )(*parts)
    return ig, gg.T, ug.T, dg.T


def solution(mesh):
    return jax.shard_map(
        per_device,
        mesh=mesh,
        in_specs=(
            P(("rep", "fs", "tp"), None),
            P(),
            P(),
            P(("rep", "fs"), "tp"),
            P(("rep", "fs"), "tp"),
            P(("rep", "fs", "tp"), None),
            P(("rep", "fs", "tp"), None),
            P("fs", "tp"),
            P("fs", "tp"),
            P("fs", "tp"),
        ),
        out_specs=(P(("rep", "fs", "tp"), None), P("fs", "tp"), P("fs", "tp"), P("fs", "tp")),
        check_vma=False,
    )
```

```python
import jax
import jax.numpy as jnp
from jax import lax
from jax.experimental import pallas as pl
from jax.experimental.pallas import tpu as pltpu
from jax.sharding import PartitionSpec as P

MESH = pl.DeviceIdType.MESH
bf16, f32 = jnp.bfloat16, jnp.float32
eps = 1e-06

HU = 352
QU = HU // 2
NQ = (128, 192, 192)
N_RECV, N_SEND, N_LOCAL = 108, 64, 20
ORDER = (
    2, 21, 0, 38, 3, 12, 47, 1, 30, 25, 23, 7, 4, 46, 16, 13, 40, 39, 24, 27, 14, 17, 8, 15, 41, 22,
    28, 31, 42, 43, 5, 19, 26, 6, 9, 35, 44, 10, 32, 48, 45, 50, 85, 51, 52, 36, 53, 11, 49, 86, 33,
    72, 62, 18, 37, 71, 74, 34, 58, 131, 59, 54, 108, 55, 87, 56, 57, 73, 94, 60, 76, 61, 132, 20,
    75, 29, 63, 109, 88, 64, 77, 80, 118, 120, 95, 133, 117, 65, 97, 99, 110, 67, 101, 89, 96, 98,
    78, 100, 134, 122, 102, 124, 119, 66, 79, 103, 111, 121, 123, 125, 135, 90, 126, 104, 91, 81,
    136, 112, 68, 127, 105, 137, 113, 92, 82, 128, 106, 114, 83, 138, 69, 129, 107, 115, 84, 130,
    70, 116, 93, 139,
)


def mod(a, n):
    return lax.rem(a + n, n)


def kernel(
    x_hbm, pre_hbm, post_hbm, gs_hbm, us_hbm, br_hbm, oc_hbm, gw_hbm, uw_hbm, dw_hbm,
    ig_hbm, d_out, g_out, u_out,
    *scratch,
):
    s = dict(zip(SCRATCH, scratch))
    W, R, G, GU, silu, dgate, hid = (s[k] for k in ("W", "R", "G", "GU", "si", "dg", "hid"))
    cot, cotT, NG, NS, NX1, NXc = (s[k] for k in ("cot", "cotT", "NG", "NS", "NX1", "NXc"))
    NB, NC = s["NB"], s["NC"]
    RY1, RYo, S, M4, MR, T, XF, K4, KR, KS, U1, UR, TQ, XQ = (
        [s[k, m] for m in range(3)] for k in BUFS
    )
    x_ref, pre_ref, post_ref, br_ref, oc_ref, ig_ref = (
        s[k] for k in ("x", "pre", "post", "br", "oc", "ig")
    )
    ssem, rsem, lsem = s["ssem"], s["rsem"], s["lsem"]
    out = (d_out, g_out, u_out)
    rep, fs, tp = lax.axis_index("rep"), lax.axis_index("fs"), lax.axis_index("tp")
    zl, y = fs // 4, fs % 4
    z = rep * 4 + zl
    x, core = tp // 2, tp % 2
    sib = 1 - core
    half = y // 2
    mate, cross = y + 1 - 2 * (y % 2), 3 - y
    diag = 3 - mate
    zm, zp, z2 = mod(zl - 1, 4), mod(zl + 1, 4), mod(zl + 2, 4)
    xm, xp, x2 = mod(x - 1, 4), mod(x + 1, 4), mod(x + 2, 4)

    def zdev(d):
        zz = mod(z + d, 8)
        return {"rep": zz // 4, "fs": (zz % 4) * 4 + y}

    dev = {
        "m": {"fs": zl * 4 + mate},
        "c": {"fs": zl * 4 + cross},
        "z+": zdev(1),
        "z-": zdev(-1),
        "zz+": zdev(2),
        "zz-": zdev(-2),
        "x+": {"tp": xp * 2 + core},
        "x-": {"tp": xm * 2 + core},
        "s": {"tp": x * 2 + sib},
    }
    ZS = ("z+", "z-")
    XS = ("x+", "x-")

    barrier = pltpu.get_barrier_semaphore()
    for name in dev:
        pl.semaphore_signal(barrier, inc=1, device_id=dev[name], device_id_type=MESH)

    ids = {}
    sends = []
    count = [0]

    def number(key):
        return ids.setdefault(key, len(ids))

    def send(key, src, dst, to):
        if len(sends) == N_SEND:
            sends.pop(0).wait_send()
        c = pltpu.make_async_remote_copy(
            src_ref=src, dst_ref=dst, send_sem=ssem.at[count[0] % N_SEND],
            recv_sem=rsem.at[number(key)], device_id=dev[to], device_id_type=MESH,
        )
        c.start()
        count[0] += 1
        sends.append(c)

    def recv(key, ref):
        pltpu.make_async_copy(ref, ref, rsem.at[number(key)]).wait()

    own = (dw_hbm, gw_hbm, uw_hbm)
    local = {}

    def load(key, src, dst):
        c = pltpu.make_async_copy(src, dst, lsem.at[len(local)])
        c.start()
        local[key] = c

    mine = pl.ds(pl.multiple_of(half * HU, 32), HU)
    other = pl.ds(pl.multiple_of((1 - half) * HU, 32), HU)
    load("br", br_hbm, br_ref)
    load("oc", oc_hbm, oc_ref)
    load("post", post_hbm, post_ref)
    load("x", x_hbm, x_ref)
    load("pre", pre_hbm, pre_ref)
    load("gs", gs_hbm.at[mine], GU.at[0, 0])
    load("us", us_hbm.at[mine], GU.at[0, 1])
    for m in range(3):
        load(("w", m), own[m].at[mine], W.at[m, zl, y])

    def rows_b():
        for key in ("br", "oc", "post"):
            local[key].wait()
        br = br_ref[...].astype(f32)
        inv_b = lax.rsqrt(jnp.mean(br * br, axis=-1, keepdims=True) + eps)
        upst = 0.5 * oc_ref[...].astype(f32) * post_ref[...]
        mean = jnp.mean(upst * br, axis=-1, keepdims=True)
        R[1, 0, tp] = (inv_b * upst - br * (inv_b * inv_b * inv_b) * mean).astype(bf16)

    def rows_n():
        for key in ("x", "pre"):
            local[key].wait()
        xf = x_ref[...].astype(f32)
        inv_x = lax.rsqrt(jnp.mean(xf * xf, axis=-1, keepdims=True) + eps)
        R[0, 0, tp] = (xf * inv_x * pre_ref[...]).astype(bf16)

    ev = [rows_b, rows_n]

    def event(fn, *args):
        ev.append(lambda: fn(*args))

    def enter():
        pl.semaphore_wait(barrier, len(dev))

    event(enter)

    def ag_own(m):
        w = own[m].at[mine]
        send(("o", m), w, W.at[m, zl, y], "m")
        send(("c", m), own[m].at[other], W.at[m, zl, y], "c")
        for to in ZS:
            send(("z", m, 0), w, W.at[m, zl, y], to)

    def ag_y(m, k):
        yy = (mate, cross, diag)[k]
        w = W.at[m, zl, yy]
        recv((("o", m), ("c", m), ("d", m))[k], w)
        if k == 1:
            send(("d", m), w, w, "m")
        for to in ZS:
            send(("z", m, k + 1), w, w, to)

    Q = (pl.ds(0, QU), pl.ds(QU, QU))

    def ag_z(m, k):
        yy = (y, mate, cross, diag)[k]
        recv(("z", m, k), W.at[m, 0, pl.ds(0, 2)])
        for d in range(2):
            w = W.at[m, (zm, zp)[d], yy, Q[d]]
            send(("w", m), w, w, ZS[d])

    def ag_end(m):
        local[("w", m)].wait()
        recv(("w", m), W.at[m, z2])

    for m in range(3):
        event(ag_own, m)
        for k in range(3):
            event(ag_y, m, k)
        for k in range(4):
            event(ag_z, m, k)
        event(ag_end, m)

    C = (pl.ds(0, 1024), pl.ds(1024, 1024))

    def rows_own(n):
        r = R.at[n, 0, tp]
        send(("rc", n), r, R.at[n, 1, tp], "c")
        rows_out(n, 0)

    def rows_cross(n):
        recv(("rc", n), R.at[n, 1, tp])
        rows_out(n, 1)

    def rows_out(n, b):
        r = R.at[n, b, tp]
        for to in XS:
            send(("r", n, b), r, r, to)
        send(("j", n, b), r, r, "s")

    def rows_near(n, b):
        recv(("r", n, b), R.at[n, b, pl.ds(0, 2)])
        for d in range(2):
            slot = (xm, xp)[d] * 2 + core
            r = R.at[n, b, slot, :, C[d]]
            send(("rf", n, b), r, r, XS[d])
        for d in range(2):
            r = R.at[n, b, (xm, xp)[d] * 2 + core]
            send(("j", n, b), r, r, "s")

    def rows_far(n, b):
        r = R.at[n, b, x2 * 2 + core]
        recv(("rf", n, b), r)
        send(("j", n, b), r, r, "s")

    def rows_end(n, b):
        recv(("j", n, b), R.at[n, b, pl.ds(0, 4)])

    for n in range(2):
        event(rows_own, n)
        event(rows_cross, n)
        for b in range(2):
            event(rows_near, n, b)
            event(rows_far, n, b)
            event(rows_end, n, b)

    def gates_out():
        send("gu", gs_hbm.at[other], GU.at[1, 0], "c")
        send("gu", us_hbm.at[other], GU.at[1, 1], "c")

    def factors(b):
        if b == 0:
            local["gs"].wait()
            local["us"].wait()
        else:
            recv("gu", GU.at[1])
        cols = pl.ds(b * 512, 512)

        def body(i, _):
            r = pl.ds(pl.multiple_of(i * 32, 32), 32)
            g, u = GU[b, 0, r, :].astype(f32), GU[b, 1, r, :].astype(f32)
            sg = jax.nn.sigmoid(g)
            v = g * sg
            silu[r, cols] = v
            hid[r, cols] = (v * u).astype(bf16)
            dgate[r, cols] = u * sg * (1.0 + g * (1.0 - sg))
            return 0

        lax.fori_loop(0, HU // 32, body, 0)

    CH = (zl, zm, zp, z2)

    def partial(m, c):
        n, left = ((1, hid), (0, cot.at[:HU]), (0, cot.at[HU:]))[m]
        cols = pl.ds(pl.multiple_of(CH[c] * 512, 512), 512)
        right = R[n, :, :, :, cols].reshape(1024, 512)
        g = jnp.dot(left[...], right, preferred_element_type=f32).astype(bf16)
        for k in range(4):
            G[m, CH[c], k] = g[:, k * 128 : (k + 1) * 128]
        send(("a", m, c), G.at[m, CH[c], diag, pl.ds(0, HU - NQ[m])], RY1[m].at[c], "m")

    def hidden_grad():
        def body(t, _):
            right = R[1, t].reshape(512, 2048)
            left = jnp.concatenate([W[0, k // 4, k % 4] for k in range(16)], axis=1)
            hg = lax.dot_general(
                left, right, (((1,), (1,)), ((), ())), preferred_element_type=f32
            )
            cols = pl.ds(pl.multiple_of(t * 512, 512), 512)
            cot[pl.ds(0, HU), cols] = (hg * dgate[:, cols]).astype(bf16)
            cot[pl.ds(HU, HU), cols] = (hg * silu[:, cols]).astype(bf16)
            return 0

        lax.fori_loop(0, 2, body, 0)

    def turn():
        for k in range(8):
            cotT[k * 128 : (k + 1) * 128, :] = cot[:, k * 128 : (k + 1) * 128].T

    def normed_grad(h):
        def body(c, _):
            right = jnp.concatenate(
                [jnp.concatenate([W[1, c, k], W[2, c, k]], axis=0) for k in range(4)], axis=1
            )
            g = jnp.dot(cotT[...], right, preferred_element_type=f32).astype(bf16)
            cols = pl.ds(pl.multiple_of(c * 512, 512), 512)
            NG[:, :, :, :, cols] = g.reshape(2, 4, 2, 64, 512)
            return 0

        lax.fori_loop(2 * h, 2 * h + 2, body, 0)
        send(("np", h), NG.at[:, :, sib, :, C[h]], NS.at[:, :, :, C[h]], "s")

    event(gates_out)
    event(factors, 0)
    event(factors, 1)
    event(hidden_grad)
    for m in range(3):
        for c in range(4):
            event(partial, m, c)
    event(turn)
    event(normed_grad, 0)
    event(normed_grad, 1)

    def ng_first(h):
        recv(("np", h), NS.at[:, :, :, C[h]])
        for b in range(2):
            for k in range(4):
                NG[b, k, core, :, C[h]] = NG[b, k, core, :, C[h]] + NS[b, k, :, C[h]]
        send(("n1", h), NG.at[:, x2, core, :, C[h]], NX1.at[h], XS[h])
        send("n", NG.at[:, (xm, xp)[h], core, :, C[h]], NXc.at[2 + h], XS[1 - h])

    def ng_second(h):
        nxt = (xp, xm)[h]
        recv(("n1", h), NX1.at[h])
        for b in range(2):
            NG[b, nxt, core, :, C[h]] = NG[b, nxt, core, :, C[h]] + NX1[h, b]
        send("n", NG.at[:, nxt, core, :, C[h]], NXc.at[h], XS[h])

    def ng_sum(b):
        return jnp.concatenate(
            [
                NG[b, x, core, :, C[h]].astype(f32)
                + NXc[h, b].astype(f32)
                + NXc[2 + h, b].astype(f32)
                for h in range(2)
            ],
            axis=1,
        )

    def ng_third():
        recv("n", NXc)
        NB[...] = ng_sum(1).astype(bf16)
        send("nc", NB, NC, "c")

    def ng_end():
        recv("nc", NC)
        w = (ng_sum(0) + NC[...].astype(f32)) * pre_ref[...]
        xv = x_ref[...].astype(f32)
        inv = lax.rsqrt(jnp.mean(xv * xv, axis=-1, keepdims=True) + eps)
        ig_ref[...] = (
            oc_ref[...].astype(f32)
            + inv * w
            - xv * (inv * inv * inv) * jnp.mean(w * xv, axis=-1, keepdims=True)
        ).astype(bf16)
        load("ig", ig_ref, ig_hbm)

    for h in range(2):
        event(ng_first, h)
        event(ng_second, h)
    event(ng_third)
    event(ng_end)

    OWN = {k: (mod(zl + k, 4), mod(z + k, 8) // 4) for k in (4, 3, 2, 1, -1, -2, -3)}

    def add3(a, b, c):
        return (a.astype(f32) + b.astype(f32) + c.astype(f32)).astype(bf16)

    def from_rep(d):
        return mod(z + (-2, 2)[d], 8) // 4

    def rs_first(m):
        p = pl.ds(0, HU - NQ[m])
        for c in range(4):
            send(("C", m, c), G.at[m, CH[c], mate, p], RYo[m].at[c], "m")

    def rs_second(m, c):
        p = pl.ds(0, HU - NQ[m])
        recv(("a", m, c), RY1[m].at[c])
        G[m, CH[c], cross, p] = G[m, CH[c], cross, p] + RY1[m][c]
        send(("C", m, c), G.at[m, CH[c], cross, p], S[m].at[CH[c], half], "c")

    def rs_third(m, c):
        p = pl.ds(0, HU - NQ[m])
        recv(("C", m, c), S[m].at[CH[c]])
        S[m][CH[c], half] = G[m, CH[c], y, p] + RYo[m][c]
        if c == 0:
            slot, h = OWN[4]
            for d in range(2):
                send(("M", m, 4), S[m].at[slot, h, part(m, d)], M4[m].at[d], ZS[d])

    def part(m, d):
        n = (HU - NQ[m]) // 2
        return pl.ds(d * n, n)

    def rs_ring(m, k):
        recv(("M", m, k + 1), M4[m] if k == 3 else MR[m].at[2 - k])
        for d in range(2):
            slot, h = OWN[(k, -k)[d]]
            if k == 3:
                r = part(m, d)
                S[m][slot, h, r] = S[m][slot, h, r] + M4[m][d]
            else:
                S[m][slot, h] = S[m][slot, h] + MR[m][2 - k, d]
            send(("M", m, k), S[m].at[slot, h], MR[m].at[3 - k, d], ZS[d])

    def rows_at(start, n):
        return pl.ds(pl.multiple_of(start, 16), n)

    def rs_own(m):
        recv(("M", m, 1), MR[m].at[2])
        T[m][...] = add3(S[m][zl, rep], MR[m][2, 0], MR[m][2, 1])
        for d in range(2):
            r = part(m, d)
            send(("x", m), T[m].at[r], XF[m].at[r], ("zz+", "zz-")[d])
        load(("out", m), T[m], out[m].at[rows_at(rep * HU, HU - NQ[m])])

    def rs_swap(m):
        recv(("x", m), XF[m])
        n = (HU - NQ[m]) // 2
        for d in range(2):
            dst = out[m].at[rows_at(from_rep(d) * HU + d * n, n)]
            send(("e", m), XF[m].at[part(m, d)], dst, ("zz+", "zz-")[d])

    def rows_q(m, h, d, parts):
        n = NQ[m]
        return rows_at(HU - n + h * (n // 2) + d * (n // 4), n // parts)

    def qs_first(m):
        slot, h = OWN[4]
        for d in range(2):
            send(("K", m, 4), G.at[m, slot, :, rows_q(m, h, d, 4)], K4[m].at[d], ZS[d])

    def qs_ring(m, k):
        recv(("K", m, k + 1), K4[m] if k == 3 else KR[m].at[2 - k])
        for d in range(2):
            slot, h = OWN[(k, -k)[d]]
            if k == 3:
                r = rows_q(m, h, d, 4)
                G[m, slot, :, r] = G[m, slot, :, r] + K4[m][d]
            else:
                r = rows_q(m, h, 0, 2)
                G[m, slot, :, r] = G[m, slot, :, r] + KR[m][2 - k, d]
            src = G.at[m, slot, :, rows_q(m, h, 0, 2)]
            send(("K", m, k), src, KR[m].at[3 - k, d], ZS[d])

    def qs_own(m):
        recv(("K", m, 1), KR[m].at[2])
        KS[m][...] = add3(G[m, zl, :, rows_q(m, rep, 0, 2)], KR[m][2, 0], KR[m][2, 1])
        send(("u", m), KS[m].at[diag], U1[m], "m")
        send(("U", m), KS[m].at[mate], UR[m].at[0], "m")

    def qs_cross(m):
        recv(("u", m), U1[m])
        KS[m][cross] = KS[m][cross] + U1[m][...]
        send(("U", m), KS[m].at[cross], UR[m].at[1], "c")

    def qs_sum(m):
        recv(("U", m), UR[m])
        TQ[m][half] = KS[m][y] + UR[m][0]
        TQ[m][1 - half] = UR[m][1]
        n = NQ[m] // 2
        for d in range(2):
            send(("v", m), TQ[m].at[d], XQ[m].at[d], ("zz+", "zz-")[d])
            load(("out", m, d), TQ[m].at[d], out[m].at[rows_at((d + 1) * HU - 2 * n + rep * n, n)])

    def qs_swap(m):
        recv(("v", m), XQ[m])
        n = NQ[m] // 2
        for d in range(2):
            dst = out[m].at[rows_at((d + 1) * HU - 2 * n + from_rep(d) * n, n)]
            send(("e", m), XQ[m].at[d], dst, ("zz+", "zz-")[d])

    def rs_end(m):
        recv(("e", m), G.at[m, 0, 0])

    for m in range(3):
        event(rs_first, m)
        for c in range(4):
            event(rs_second, m, c)
            event(rs_third, m, c)
        for k in (3, 2, 1):
            event(rs_ring, m, k)
        event(rs_own, m)
        event(rs_swap, m)
        event(qs_first, m)
        for k in (3, 2, 1):
            event(qs_ring, m, k)
        event(qs_own, m)
        event(qs_cross, m)
        event(qs_sum, m)
        event(qs_swap, m)
        event(rs_end, m)

    for k in ORDER:
        ev[k]()
    assert sorted(ORDER) == list(range(len(ev))) and len(ids) <= N_RECV
    for c in sends:
        c.wait_send()
    for key in local:
        if key == "ig" or key[0] == "out":
            local[key].wait()


V, SEM = pltpu.VMEM, pltpu.SemaphoreType.DMA
SCRATCH = {
    "W": V((3, 4, 4, HU, 128), bf16),
    "R": V((2, 2, 8, 64, 2048), bf16),
    "G": V((3, 4, 4, HU, 128), bf16),
    "GU": V((2, 2, HU, 512), bf16),
    "si": V((HU, 1024), f32),
    "dg": V((HU, 1024), f32),
    "hid": V((HU, 1024), bf16),
    "cot": V((2 * HU, 1024), bf16),
    "cotT": V((1024, 2 * HU), bf16),
    "NG": V((2, 4, 2, 64, 2048), bf16),
    "NS": V((2, 4, 64, 2048), bf16),
    "NX1": V((2, 2, 64, 1024), bf16),
    "NXc": V((4, 2, 64, 1024), bf16),
    "NB": V((64, 2048), bf16),
    "NC": V((64, 2048), bf16),
    "x": V((64, 2048), bf16),
    "br": V((64, 2048), bf16),
    "oc": V((64, 2048), bf16),
    "ig": V((64, 2048), bf16),
    "pre": V((1, 2048), f32),
    "post": V((1, 2048), f32),
    "ssem": SEM((N_SEND,)),
    "rsem": SEM((N_RECV,)),
    "lsem": SEM((N_LOCAL,)),
}


BUFS = ("RY1", "RYo", "S", "M4", "MR", "T", "XF", "K4", "KR", "KS", "U1", "UR", "TQ", "XQ")
for m in range(3):
    p, h = HU - NQ[m], NQ[m] // 2
    shapes = (
        (4, p), (4, p), (4, 2, p), (2, p // 2), (3, 2, p), (p,), (p,),
        (2, 4, h // 2), (3, 2, 4, h), (4, h), (h,), (2, h), (2, h), (2, h),
    )
    for k, shape in zip(BUFS, shapes):
        SCRATCH[k, m] = V((*shape, 128), bf16)


def finish(*refs):
    ins, outs, (row, half, full, sem) = refs[:4], refs[4:8], refs[8:]
    bufs = [row] + [half.at[m] for m in range(3)]
    res = [row] + [full.at[m] for m in range(3)]
    loads = [pltpu.make_async_copy(ins[k], bufs[k], sem.at[k]) for k in range(4)]
    stores = [pltpu.make_async_copy(res[k], outs[k], sem.at[4 + k]) for k in range(4)]
    for c in loads:
        c.start()
    for k in range(4):
        loads[k].wait()
        if k:
            full[k - 1] = half[k - 1].astype(f32)
        stores[k].start()
    for c in stores:
        c.wait()


def per_device(x, pre, post, gs, us, br, oc, gw, uw, dw):
    hbm = pl.BlockSpec(memory_space=pl.ANY)
    sds = jax.ShapeDtypeStruct
    parts = pl.pallas_call(
        kernel,
        out_shape=(sds((64, 2048), bf16), *[sds((2 * HU, 128), bf16)] * 3),
        in_specs=[hbm] * 10,
        out_specs=(hbm,) * 4,
        scratch_shapes=list(SCRATCH.values()),
        compiler_params=pltpu.CompilerParams(
            collective_id=0, has_side_effects=True, vmem_limit_bytes=67_000_000
        ),
        name="ffn_backward",
    )(x, pre.reshape(1, -1), post.reshape(1, -1), gs.T, us.T, br, oc, gw.T, uw.T, dw.T)
    ig, dg, gg, ug = pl.pallas_call(
        finish,
        out_shape=(sds((64, 2048), bf16), *[sds((2 * HU, 128), f32)] * 3),
        in_specs=[hbm] * 4,
        out_specs=(hbm,) * 4,
        scratch_shapes=[
            V((64, 2048), bf16), V((3, 2 * HU, 128), bf16), V((3, 2 * HU, 128), f32), SEM((8,)),
        ],
        name="finish",
    )(*parts)
    return ig, gg.T, ug.T, dg.T


def solution(mesh):
    return jax.shard_map(
        per_device,
        mesh=mesh,
        in_specs=(
            P(("rep", "fs", "tp"), None),
            P(),
            P(),
            P(("rep", "fs"), "tp"),
            P(("rep", "fs"), "tp"),
            P(("rep", "fs", "tp"), None),
            P(("rep", "fs", "tp"), None),
            P("fs", "tp"),
            P("fs", "tp"),
            P("fs", "tp"),
        ),
        out_specs=(P(("rep", "fs", "tp"), None), P("fs", "tp"), P("fs", "tp"), P("fs", "tp")),
        check_vma=False,
    )
```
